32 devices in a mesh: sp: 8 (over z, y), tp: 4 (over x, core).
Axes of the slice: x: 2, y: 2, z: 4, core: 2. Of those that a mesh axis runs over, the one named last changes fastest.
Arguments:
- stream: bfloat16 [2048, 2048], P('sp'), may hold values from -6 to 6
- attn_gain: float32 [2, 2048], replicated, may hold values from 0.1 to 1.9
- w_query: bfloat16 [2, 2048, 2048], P(None, None, 'tp'), may hold values from -0.125 to 0.125
- w_key: bfloat16 [2, 2048, 512], P(None, None, 'tp'), may hold values from -0.125 to 0.125
- w_value: bfloat16 [2, 2048, 512], P(None, None, 'tp'), may hold values from -0.125 to 0.125
- w_out: bfloat16 [2, 2048, 2048], P(None, 'tp'), may hold values from -1 to 1
- query_gain: float32 [2, 64], replicated, may hold values from 0.1 to 1.9
- key_gain: float32 [2, 64], replicated, may hold values from 0.1 to 1.9
- rel_bias: float32 [2, 32, 257], P(None, 'tp'), may hold values from -6 to 300
Outputs:
- result: bfloat16 [2048, 2048], P('sp', 'tp')
The draws below stay inside these ranges and needn't reach their ends.
All inputs are finite; a program needn't handle non-finite values.
Results may differ from the reference program's by a relative error of at most 0.02.
Values may be sent and summed in bfloat16 or wider, within the bound.
No kernel may reach another device: no remote copies, remote signals or barrier semaphores. Data moves between devices by JAX's collectives and lax.ppermute only.
A program may use at most 64 MiB of HBM per device.

```python
import jax
import jax.numpy as jnp
from jax import lax

D = 2048
HEAD_DIM = 64
HEADS = 32
KV_HEADS = 8
SEG = 64
LEFT = 4
CLIP = 128
LAYERS = 2
TOKENS = 2048
N_TP = 4


def draw_rel_bias(key, part):
    subkeys = jax.random.split(jax.random.fold_in(key, 17), 1)
    shape = (LAYERS, HEADS, 2 * CLIP + 1)
    bias_table = jnp.clip(jax.random.normal(subkeys[0], shape, jnp.float32), -6.0, 6.0)
    return bias_table


def shard_levels(key, extent, cuts, least, high):
    level = 1.0
    for dim, parts in cuts:
        steps = jax.random.uniform(jax.random.fold_in(jax.random.fold_in(key, 6), dim), (parts,), jnp.float32, least / len(cuts), high / len(cuts))
        level = level * jnp.repeat(jnp.exp(steps), extent[dim] // parts).reshape((-1,) + (1,) * (len(extent) - 1 - dim))
    return level


def scatter_about(stream_key, extent, scale, bound, cuts=(), held_as=jnp.bfloat16):
    result = jax.random.normal(stream_key, extent, jnp.float32) * scale
    if len(cuts) > 0:
        result = shard_levels(stream_key, extent, cuts, -0.22, 0.18) * result
    return jnp.clip(result, min=-bound, max=bound).astype(held_as)


def setup_inputs(seed: int = 0) -> dict:
    arg_keys = jax.random.split(jax.random.key(seed), 10)
    return {
        "stream": scatter_about(arg_keys[0], (TOKENS, D), 1.0, 6.0, ((0, 8),)),
        "attn_gain": jnp.clip(1.0 + 0.18 * jax.random.normal(arg_keys[1], (LAYERS, D), jnp.float32), 0.1, 1.9),
        "w_query": scatter_about(arg_keys[2], (LAYERS, D, D), D ** -0.5, 0.125, ((2, 4),)),
        "w_key": scatter_about(arg_keys[3], (LAYERS, D, KV_HEADS * HEAD_DIM), D ** -0.5, 0.125, ((2, 4),)),
        "w_value": scatter_about(arg_keys[4], (LAYERS, D, KV_HEADS * HEAD_DIM), D ** -0.5, 0.125, ((2, 4),)),
        "w_out": scatter_about(arg_keys[5], (LAYERS, D, D), (D // 64) ** -0.5, 1.0, ((1, 4),)),
        "query_gain": jnp.clip(1.0 + 0.18 * jax.random.normal(arg_keys[6], (LAYERS, HEAD_DIM), jnp.float32), 0.1, 1.9),
        "key_gain": jnp.clip(1.0 + 0.18 * jax.random.normal(arg_keys[7], (LAYERS, HEAD_DIM), jnp.float32), 0.1, 1.9),
        "rel_bias": draw_rel_bias(jax.random.fold_in(arg_keys[9], 71), 0),
    }


norm_eps = 1e-06
masked_score = -1e+30

def rms_scale(values_in, gain):
    squared = lax.optimization_barrier(jnp.mean(values_in * values_in, axis=-1, keepdims=True))
    return values_in * lax.rsqrt(squared + norm_eps) * gain

def bias_block(bias_table, key_reach):
    query_pos = jnp.arange(key_reach, dtype=jnp.int32)[:, None]
    key_pos = jnp.arange(2 * key_reach, dtype=jnp.int32)[None, :]
    distance = jnp.clip(query_pos + key_reach - key_pos, -CLIP, CLIP) + CLIP
    return bias_table[:, distance].astype(jnp.float32)

def band_mask(key_reach, first_query):
    query_pos = jnp.arange(key_reach, dtype=jnp.int32)[:, None]
    key_pos = jnp.arange(2 * key_reach, dtype=jnp.int32)[None, :] - key_reach
    query_seg = query_pos // SEG
    key_seg = key_pos // SEG
    return (key_seg <= query_seg) & (key_seg >= query_seg - LEFT) & (first_query + key_pos >= 0)

def band_attention(queries, keys_all, values_all, bias_table):
    key_reach = LEFT * SEG
    group = HEADS // KV_HEADS
    total_rows = queries.shape[0]
    bias = bias_block(bias_table, key_reach).reshape(KV_HEADS, group, key_reach, 2 * key_reach)

    def one_block(block_index):
        start = block_index * key_reach
        query_rows = lax.dynamic_slice_in_dim(queries, start, key_reach, 0).reshape(key_reach, KV_HEADS, group, HEAD_DIM)
        key_rows = lax.dynamic_slice_in_dim(keys_all, start, 2 * key_reach, 0)
        value_rows = lax.dynamic_slice_in_dim(values_all, start, 2 * key_reach, 0)
        scores = jnp.einsum('qkgd,jkd->kgqj', query_rows.astype(jnp.float32), key_rows.astype(jnp.float32)) * HEAD_DIM ** (-0.5) + bias
        inside = band_mask(key_reach, start)
        scores = jnp.where(inside, scores, masked_score)
        peak = lax.optimization_barrier(jnp.max(scores, axis=-1, keepdims=True))
        expon = jnp.exp(scores - peak)
        weights = lax.optimization_barrier((expon / lax.optimization_barrier(jnp.sum(expon, axis=-1, keepdims=True))).astype(jnp.bfloat16))
        mixed = jnp.einsum('kgqj,jkd->qkgd', weights.astype(jnp.float32), value_rows.astype(jnp.float32))
        return mixed.astype(jnp.bfloat16).reshape(key_reach, HEADS * HEAD_DIM)
    blocks = lax.map(one_block, jnp.arange(total_rows // key_reach, dtype=jnp.int32))
    return blocks.reshape(total_rows, HEADS * HEAD_DIM)

def reference(stream, attn_gain, w_query, w_key, w_value, w_out, query_gain, key_gain, rel_bias):
    current = stream
    total_rows = stream.shape[0]
    key_reach = LEFT * SEG
    head_cols = D // N_TP
    for layer_index in range(LAYERS):
        normed = rms_scale(current.astype(jnp.float32), attn_gain[layer_index]).astype(jnp.bfloat16)
        query_flat = jnp.dot(normed, w_query[layer_index], preferred_element_type=jnp.float32)
        queries = rms_scale(query_flat.reshape(total_rows, HEADS, HEAD_DIM), query_gain[layer_index]).astype(jnp.bfloat16)
        key_flat = jnp.dot(normed, w_key[layer_index], preferred_element_type=jnp.float32)
        keys_now = rms_scale(key_flat.reshape(total_rows, KV_HEADS, HEAD_DIM), key_gain[layer_index]).astype(jnp.bfloat16)
        values_now = jnp.dot(normed, w_value[layer_index], preferred_element_type=jnp.float32).astype(jnp.bfloat16).reshape(total_rows, KV_HEADS, HEAD_DIM)
        padding = jnp.zeros((key_reach, KV_HEADS, HEAD_DIM), jnp.bfloat16)
        keys_all = jnp.concatenate([padding, keys_now], axis=0)
        values_all = jnp.concatenate([padding, values_now], axis=0)
        mixed = band_attention(queries, keys_all, values_all, rel_bias[layer_index])
        update = jnp.zeros((total_rows, D), jnp.float32)
        for group_index in range(N_TP):
            lower = group_index * head_cols
            partial_value = jnp.dot(mixed[:, lower:lower + head_cols], w_out[layer_index, lower:lower + head_cols], preferred_element_type=jnp.float32)
            update = update + lax.optimization_barrier(partial_value.astype(jnp.bfloat16)).astype(jnp.float32)
        current = (current.astype(jnp.float32) + update).astype(jnp.bfloat16)
    return current
```

```python
import functools

import jax
import jax.numpy as jnp
from jax import lax
from jax.experimental import pallas as pl
from jax.experimental.pallas import tpu as pltpu
from jax.sharding import PartitionSpec as P

HEAD_DIM = 64
SEG = 64
LEFT = 4
CLIP = 128
LAYERS = 2

REACH = LEFT * SEG
CHUNK = 2 * SEG
WINDOW = REACH + CHUNK
LINE = WINDOW + CHUNK
LANES = 128

norm_eps = 1e-06
masked_score = -1e30

bf16 = jnp.bfloat16
f32 = jnp.float32

whole = pl.BlockSpec(memory_space=pltpu.VMEM)
scalar = pl.BlockSpec(memory_space=pltpu.SMEM)
anywhere = pl.BlockSpec(memory_space=pl.ANY)


def params():
    return pltpu.CompilerParams(vmem_limit_bytes=24 * 1024 * 1024)


def fetch(source_ref, target_ref, sems, layer_index):
    share = target_ref.shape[0] // sems.shape[0]
    copies = []
    for index in range(sems.shape[0]):
        at = pl.ds(index * share, share)
        copy = pltpu.make_async_copy(
            source_ref.at[layer_index, at, :], target_ref.at[at, :], sems.at[index]
        )
        copy.start()
        copies.append(copy)
    return copies


def cost(flops, moved):
    return pl.CostEstimate(flops=int(flops), bytes_accessed=int(moved), transcendentals=0)


def head_norm(flat, gain_row):
    width = flat.shape[1]
    step = min(width, LANES)
    row = lax.broadcasted_iota(jnp.int32, (step, step), 0) // HEAD_DIM
    col = lax.broadcasted_iota(jnp.int32, (step, step), 1) // HEAD_DIM
    mean_of = jnp.where(row == col, 1.0 / HEAD_DIM, 0.0).astype(bf16)
    gain = jnp.concatenate([gain_row] * (step // HEAD_DIM), axis=1)
    pieces = []
    for lower in range(0, width, step):
        part = flat[:, lower : lower + step]
        squared = part * part
        high = squared.astype(bf16)
        low = (squared - high.astype(f32)).astype(bf16)
        mean = jnp.dot(high, mean_of, preferred_element_type=f32) + jnp.dot(
            low, mean_of, preferred_element_type=f32
        )
        pieces.append(part * lax.rsqrt(mean + norm_eps) * gain)
    return pieces


def key_value_body(normed, wk_ref, wv_ref, key_gain_ref, layer_index, kv_ref, copies):
    for copy in copies:
        copy.wait()
    keys = jnp.dot(normed, wk_ref[...], preferred_element_type=f32)
    values = jnp.dot(normed, wv_ref[...], preferred_element_type=f32)
    keys = head_norm(keys, key_gain_ref[layer_index : layer_index + 1, :])[0]
    kv_ref[...] = jnp.concatenate([keys, values], axis=1).astype(bf16)


def first_norm_kernel(
    layer_index, x_ref, gain_ref, wk_any, wv_any, kg_ref, normed_ref, kv_ref,
    wk_ref, wv_ref, sems,
):
    copies = fetch(wk_any, wk_ref, sems.at[0:1], layer_index)
    copies += fetch(wv_any, wv_ref, sems.at[1:2], layer_index)
    current = x_ref[...].astype(f32)
    mean = jnp.mean(current * current, axis=-1, keepdims=True)
    gain = gain_ref[layer_index : layer_index + 1, :]
    normed_ref[...] = (current * lax.rsqrt(mean + norm_eps) * gain).astype(bf16)
    key_value_body(normed_ref[...], wk_ref, wv_ref, kg_ref, layer_index, kv_ref, copies)


def next_norm_kernel(
    layer_index, block, place_ref, mine_ref, other_ref, gain_ref, wk_any, wv_any, kg_ref,
    normed_ref, kv_ref, wk_ref, wv_ref, sems,
):
    copies = fetch(wk_any, wk_ref, sems.at[0:1], layer_index)
    copies += fetch(wv_any, wv_ref, sems.at[1:2], layer_index)
    parity = place_ref[1]
    mine = mine_ref[...].astype(f32)
    other = other_ref[...].astype(f32)
    total = jnp.sum(mine * mine, axis=-1, keepdims=True)
    total = total + jnp.sum(other * other, axis=-1, keepdims=True)
    scale = lax.rsqrt(total / (2 * mine.shape[1]) + norm_eps)
    for index in range(mine.shape[1] // block):
        for held, side in ((mine, parity), (other, 1 - parity)):
            cols = pl.ds(pl.multiple_of((2 * index + side) * block, LANES), block)
            piece = held[:, index * block : (index + 1) * block]
            gain = gain_ref[layer_index : layer_index + 1, cols]
            normed_ref[:, cols] = (piece * scale * gain).astype(bf16)
    key_value_body(normed_ref[...], wk_ref, wv_ref, kg_ref, layer_index, kv_ref, copies)


def query_kernel(layer_index, normed_ref, wq_any, qg_ref, q_ref, wq_ref, sems):
    copies = fetch(wq_any, wq_ref, sems, layer_index)
    share = wq_ref.shape[0] // len(copies)
    flat = None
    for index, copy in enumerate(copies):
        copy.wait()
        at = slice(index * share, (index + 1) * share)
        part = jnp.dot(normed_ref[:, at], wq_ref[at, :], preferred_element_type=f32)
        flat = part if flat is None else flat + part
    pieces = head_norm(flat, qg_ref[layer_index : layer_index + 1, :])
    width = pieces[0].shape[1]
    for index, piece in enumerate(pieces):
        scaled = piece.astype(bf16) * bf16(HEAD_DIM**-0.5)
        q_ref[:, index * width : (index + 1) * width] = scaled


def bias_kernel(table_ref, tile_ref):
    layers, heads, entries = table_ref.shape
    source = lax.broadcasted_iota(jnp.int32, (entries, LINE), 0)
    offset = lax.broadcasted_iota(jnp.int32, (entries, LINE), 1)
    distance = jnp.clip(WINDOW - 1 - offset, -CLIP, CLIP) + CLIP
    onehot = (source == distance).astype(f32)
    query_seg = lax.broadcasted_iota(jnp.int32, (CHUNK, WINDOW), 0) // SEG
    key_seg = lax.broadcasted_iota(jnp.int32, (CHUNK, WINDOW), 1) // SEG
    inside = (key_seg >= query_seg) & (key_seg <= query_seg + LEFT)
    for layer_index in range(layers):
        line = jnp.dot(
            table_ref[layer_index], onehot, precision=lax.Precision.HIGHEST,
            preferred_element_type=f32,
        )
        for head in range(heads):
            spread = jnp.broadcast_to(line[head : head + 1, :], (CHUNK, LINE))
            rolled = pltpu.roll(spread, LINE - CHUNK + 1, 1, stride=1, stride_axis=0)
            tile_ref[layer_index, head] = jnp.where(inside, rolled[:, :WINDOW], masked_score)


def attention_kernel(
    block, layer_index, place_ref, q_ref, kv_ref, kvp_ref, tile_any, wout_any, keep_ref, send_ref,
    keys_ref, even_ref, odd_ref, mixed_ref, tile_ref, wout_ref, sems,
):
    tile_copy = pltpu.make_async_copy(tile_any.at[layer_index], tile_ref, sems.at[0])
    tile_copy.start()
    copies = fetch(wout_any, wout_ref, sems.at[1:2], layer_index)
    first, parity = place_ref[0], place_ref[1]
    rows = q_ref.shape[0]
    heads = q_ref.shape[1] // HEAD_DIM
    kv_width = kv_ref.shape[1] // 2
    kv_heads = kv_width // HEAD_DIM
    group = heads // kv_heads
    pairs = group // 2

    for part_ref, start in ((kvp_ref, 0), (kv_ref, REACH)):
        count = part_ref.shape[0]
        low = lax.broadcasted_iota(jnp.int32, (count, LANES), 1) < HEAD_DIM
        for kv in range(kv_heads):
            at = kv * HEAD_DIM
            key = part_ref[:, at : at + HEAD_DIM].astype(f32)
            value = part_ref[:, kv_width + at : kv_width + at + HEAD_DIM].astype(f32)
            key = jnp.concatenate([key, key], axis=1)
            value = jnp.concatenate([value, value], axis=1)
            keys_ref[kv, start : start + count, :] = key.astype(bf16)
            even_ref[kv, start : start + count, :] = jnp.where(low, value, 1.0).astype(bf16)
            odd_ref[kv, start : start + count, :] = jnp.where(low, 1.0, value).astype(bf16)

    tile_copy.wait()
    low = lax.broadcasted_iota(jnp.int32, (CHUNK, LANES), 1) < HEAD_DIM
    for chunk in range(rows // CHUNK):
        start = chunk * CHUNK
        key_index = start + lax.broadcasted_iota(jnp.int32, (1, WINDOW), 1)
        outside = (key_index < REACH) & (first == 1)
        outside = jnp.where(outside, masked_score, 0.0)
        for kv in range(kv_heads):
            evens, odds = [], []
            for pair in range(pairs):
                at = (kv * pairs + pair) * LANES
                both = q_ref[start : start + CHUNK, at : at + LANES]
                evens.append(jnp.where(low, both, jnp.zeros_like(both)))
                odds.append(jnp.where(low, jnp.zeros_like(both), both))
            stacked = jnp.concatenate(evens + odds, axis=0)
            window = slice(start, start + WINDOW)
            scores = lax.dot_general(
                stacked, keys_ref[kv, window, :], (((1,), (1,)), ((), ())),
                preferred_element_type=f32,
            )
            expons = []
            for index in range(group):
                pair, side = index % pairs, index // pairs
                head = kv * group + 2 * pair + side
                score = scores[index * CHUNK : (index + 1) * CHUNK, :] + tile_ref[head]
                score = score + outside
                peak = jnp.max(score, axis=-1, keepdims=True)
                expons.append(jnp.exp(score - peak).astype(bf16))
            even = jnp.dot(
                jnp.concatenate(expons[:pairs], axis=0), even_ref[kv, window, :],
                preferred_element_type=f32,
            )
            odd = jnp.dot(
                jnp.concatenate(expons[pairs:], axis=0), odd_ref[kv, window, :],
                preferred_element_type=f32,
            )
            for pair in range(pairs):
                at = (kv * pairs + pair) * LANES
                upper = even[pair * CHUNK : (pair + 1) * CHUNK, :]
                lower = odd[pair * CHUNK : (pair + 1) * CHUNK, :]
                total = pltpu.roll(jnp.where(low, lower, upper), HEAD_DIM, 1)
                mixed_ref[start : start + CHUNK, at : at + LANES] = (
                    jnp.where(low, upper, lower) / total
                ).astype(bf16)

    mixed = mixed_ref[...]
    for copy in copies:
        copy.wait()
    for index in range(keep_ref.shape[1] // block):
        for target, side in ((send_ref, 1 - parity), (keep_ref, parity)):
            cols = pl.ds(pl.multiple_of((2 * index + side) * block, LANES), block)
            partial_value = jnp.dot(mixed, wout_ref[:, cols], preferred_element_type=f32)
            target[:, index * block : (index + 1) * block] = partial_value.astype(bf16)


def add_kernel(a_ref, b_ref, out_ref):
    out_ref[...] = (a_ref[...].astype(f32) + b_ref[...].astype(f32)).astype(bf16)


def split_add_kernel(block, bit, place_ref, a_ref, b_ref, keep_ref, send_ref):
    parity = place_ref[bit]
    for index in range(keep_ref.shape[1] // block):
        into = slice(index * block, (index + 1) * block)
        for target, side in ((send_ref, 1 - parity), (keep_ref, parity)):
            cols = pl.ds(pl.multiple_of((2 * index + side) * block, LANES), block)
            target[:, into] = (
                a_ref[:, cols].astype(f32) + b_ref[:, cols].astype(f32)
            ).astype(bf16)


def residual_kernel(block, stride, bit, place_ref, x_ref, a_ref, b_ref, out_ref):
    for index in range(out_ref.shape[1] // block):
        into = slice(index * block, (index + 1) * block)
        cols = pl.ds(pl.multiple_of((stride * index + place_ref[bit]) * block, LANES), block)
        added = a_ref[:, into].astype(f32) + b_ref[:, into].astype(f32)
        out_ref[:, into] = (x_ref[:, cols].astype(f32) + added).astype(bf16)


def swapped(value, bit):
    size = lax.axis_size("tp")
    return lax.ppermute(value, "tp", [(d, d ^ (1 << bit)) for d in range(size)])


def local(stream, attn_gain, w_query, w_key, w_value, w_out, query_gain, key_gain, rel_bias):
    rows, width = stream.shape
    tp_size = lax.axis_size("tp")
    sp_size = lax.axis_size("sp")
    bits = tp_size.bit_length() - 1
    block = width // tp_size
    half = width // 2
    query_width = w_query.shape[2]
    kv_width = w_key.shape[2]
    heads = query_width // HEAD_DIM
    kv_heads = kv_width // HEAD_DIM
    tp_index = lax.axis_index("tp")
    sp_index = lax.axis_index("sp")
    place = jnp.stack(
        [(sp_index == 0).astype(jnp.int32), tp_index % 2]
        + [(tp_index >> bit) & 1 for bit in range(1, bits)]
        + [tp_index // 2]
    ).astype(jnp.int32)

    def out(shape, dtype=bf16):
        return jax.ShapeDtypeStruct(shape, dtype)

    tiles = pl.pallas_call(
        bias_kernel,
        out_shape=out((LAYERS, heads, CHUNK, WINDOW), f32),
        in_specs=[whole],
        out_specs=whole,
        compiler_params=params(),
        cost_estimate=cost(2e9, 1e6),
        name="bias_tiles",
    )(rel_bias)

    mine = other = None
    for layer_index in range(LAYERS):
        weights = (attn_gain, w_key, w_value, key_gain)
        weight_specs = [whole, anywhere, anywhere, whole]
        weight_scratch = [
            pltpu.VMEM((width, kv_width), bf16),
            pltpu.VMEM((width, kv_width), bf16),
            pltpu.SemaphoreType.DMA((2,)),
        ]
        norm_out = [out((rows, width)), out((rows, 2 * kv_width))]
        norm_cost = cost(4 * rows * width * kv_width, 4 * rows * width + 4 * width * kv_width)
        if layer_index == 0:
            normed, kv = pl.pallas_call(
                functools.partial(first_norm_kernel, layer_index),
                out_shape=norm_out,
                in_specs=[whole] + weight_specs,
                out_specs=[whole, whole],
                scratch_shapes=weight_scratch,
                compiler_params=params(),
                cost_estimate=norm_cost,
                name="norm_kv_first",
            )(stream, *weights)
        else:
            normed, kv = pl.pallas_call(
                functools.partial(next_norm_kernel, layer_index, block),
                out_shape=norm_out,
                in_specs=[scalar, whole, whole] + weight_specs,
                out_specs=[whole, whole],
                scratch_shapes=weight_scratch,
                compiler_params=params(),
                cost_estimate=norm_cost,
                name="norm_kv_next",
            )(place, mine, other, *weights)
        kv_prior = lax.ppermute(
            kv[rows - REACH :], "sp", [(d, d + 1) for d in range(sp_size - 1)]
        )
        queries = pl.pallas_call(
            functools.partial(query_kernel, layer_index),
            out_shape=out((rows, query_width)),
            in_specs=[whole, anywhere, whole],
            out_specs=whole,
            scratch_shapes=[
                pltpu.VMEM((width, query_width), bf16),
                pltpu.SemaphoreType.DMA((4,)),
            ],
            compiler_params=params(),
            cost_estimate=cost(2 * rows * width * query_width, 2 * width * query_width),
            name="queries",
        )(normed, w_query, query_gain)
        keep, send = pl.pallas_call(
            functools.partial(attention_kernel, block, layer_index),
            out_shape=[out((rows, half)), out((rows, half))],
            in_specs=[scalar, whole, whole, whole, anywhere, anywhere],
            out_specs=[whole, whole],
            scratch_shapes=[
                pltpu.VMEM((kv_heads, REACH + rows, LANES), bf16),
                pltpu.VMEM((kv_heads, REACH + rows, LANES), bf16),
                pltpu.VMEM((kv_heads, REACH + rows, LANES), bf16),
                pltpu.VMEM((rows, query_width), bf16),
                pltpu.VMEM((heads, CHUNK, WINDOW), f32),
                pltpu.VMEM((query_width, width), bf16),
                pltpu.SemaphoreType.DMA((2,)),
            ],
            compiler_params=params(),
            cost_estimate=cost(
                2 * rows * query_width * (width + 4 * WINDOW), 2 * width * query_width
            ),
            name="attention",
        )(place, queries, kv, kv_prior, tiles, w_out)
        received = swapped(send, 0)
        if layer_index < LAYERS - 1:
            for bit in range(1, bits):
                summed = pl.pallas_call(
                    add_kernel,
                    out_shape=out((rows, half)),
                    in_specs=[whole, whole],
                    out_specs=whole,
                    compiler_params=params(),
                    name="add",
                )(keep, received)
                keep, received = summed, swapped(summed, bit)
            mine = pl.pallas_call(
                functools.partial(residual_kernel, block, 2, 1),
                out_shape=out((rows, half)),
                in_specs=[scalar, whole, whole, whole],
                out_specs=whole,
                compiler_params=params(),
                name="residual",
            )(place, stream, keep, received)
            other = swapped(mine, 0)
        else:
            for bit in range(1, bits):
                left = keep.shape[1] // 2
                keep, send = pl.pallas_call(
                    functools.partial(split_add_kernel, block, 1 + bit),
                    out_shape=[out((rows, left)), out((rows, left))],
                    in_specs=[scalar, whole, whole],
                    out_specs=[whole, whole],
                    compiler_params=params(),
                    name="split_add",
                )(place, keep, received)
                received = swapped(send, bit)
            result = pl.pallas_call(
                functools.partial(residual_kernel, block, 1, bits + 1),
                out_shape=out((rows, block)),
                in_specs=[scalar, whole, whole, whole],
                out_specs=whole,
                compiler_params=params(),
                name="result",
            )(place, mine, keep, received)
    return result


def solution(mesh):
    return jax.shard_map(
        local,
        mesh=mesh,
        in_specs=(
            P("sp", None),
            P(),
            P(None, None, "tp"),
            P(None, None, "tp"),
            P(None, None, "tp"),
            P(None, "tp", None),
            P(),
            P(),
            P(None, "tp", None),
        ),
        out_specs=P("sp", "tp"),
        check_vma=False,
    )
```

```python
import functools

import jax
import jax.numpy as jnp
from jax import lax
from jax.experimental import pallas as pl
from jax.experimental.pallas import tpu as pltpu
from jax.sharding import PartitionSpec as P


HEAD_DIM = 64
SEG = 64
LEFT = 4
CLIP = 128
LAYERS = 2

REACH = LEFT * SEG
CHUNK = 2 * SEG
PIECES = REACH // CHUNK + 1
WINDOW = REACH + CHUNK
LINE = WINDOW + CHUNK
LANES = 128

norm_eps = 1e-06
masked_score = -1e30

bf16 = jnp.bfloat16
f32 = jnp.float32

whole = pl.BlockSpec(memory_space=pltpu.VMEM)
scalar = pl.BlockSpec(memory_space=pltpu.SMEM)
in_hbm = pl.BlockSpec(memory_space=pltpu.HBM)


def params():
    return pltpu.CompilerParams(vmem_limit_bytes=12 * 1024 * 1024)


def cost(flops, moved):
    return pl.CostEstimate(flops=int(flops), bytes_accessed=int(moved), transcendentals=0)


def out(shape, dtype=bf16):
    return jax.ShapeDtypeStruct(shape, dtype)


def head_norm(flat, gain_row):
    width = flat.shape[1]
    step = min(width, LANES)
    row = lax.broadcasted_iota(jnp.int32, (step, step), 0) // HEAD_DIM
    col = lax.broadcasted_iota(jnp.int32, (step, step), 1) // HEAD_DIM
    mean_of = jnp.where(row == col, 1.0 / HEAD_DIM, 0.0).astype(bf16)
    gain = jnp.concatenate([gain_row] * (step // HEAD_DIM), axis=1)
    pieces = []
    for lower in range(0, width, step):
        part = flat[:, lower : lower + step]
        squared = part * part
        high = squared.astype(bf16)
        low = (squared - high.astype(f32)).astype(bf16)
        mean = jnp.dot(high, mean_of, preferred_element_type=f32) + jnp.dot(
            low, mean_of, preferred_element_type=f32
        )
        pieces.append(part * lax.rsqrt(mean + norm_eps) * gain)
    return pieces


def key_value_body(normed, wk, wv, key_gain_row, kv_ref):
    keys = jnp.dot(normed, wk, preferred_element_type=f32)
    values = jnp.dot(normed, wv, preferred_element_type=f32)
    keys = head_norm(keys, key_gain_row)[0]
    kv_ref[...] = jnp.concatenate([keys, values], axis=1).astype(bf16)


def first_norm_kernel(
    x_hbm, gain_hbm, wk_hbm, wv_hbm, kg_hbm, normed_ref, kv_ref,
    x_ref, gain_ref, wk_ref, wv_ref, kg_ref, row_sems, sems,
):
    steps = row_sems.shape[0]
    share = x_ref.shape[0] // steps
    row_copies = []
    for index in range(steps):
        at = pl.ds(index * share, share)
        row_copies.append(
            pltpu.make_async_copy(x_hbm.at[at, :], x_ref.at[at, :], row_sems.at[index])
        )
    gain_copy = pltpu.make_async_copy(gain_hbm, gain_ref, sems.at[0])
    late = [
        pltpu.make_async_copy(wk_hbm.at[0], wk_ref, sems.at[1]),
        pltpu.make_async_copy(wv_hbm.at[0], wv_ref, sems.at[2]),
        pltpu.make_async_copy(kg_hbm, kg_ref, sems.at[3]),
    ]
    for copy in [gain_copy] + row_copies + late:
        copy.start()
    gain_copy.wait()
    gain = gain_ref[0:1, :]
    for index, copy in enumerate(row_copies):
        copy.wait()
        at = slice(index * share, (index + 1) * share)
        current = x_ref[at, :].astype(f32)
        mean = jnp.mean(current * current, axis=-1, keepdims=True)
        normed_ref[at, :] = (current * lax.rsqrt(mean + norm_eps) * gain).astype(bf16)
    for copy in late:
        copy.wait()
    key_value_body(normed_ref[...], wk_ref[...], wv_ref[...], kg_ref[0:1, :], kv_ref)


def next_norm_kernel(
    layer_index, block, place_ref, mine_ref, other_ref, gain_ref, wk_ref, wv_ref, kg_ref,
    normed_ref, kv_ref,
):
    parity = place_ref[1]
    mine = mine_ref[...].astype(f32)
    other = other_ref[...].astype(f32)
    total = jnp.sum(mine * mine, axis=-1, keepdims=True)
    total = total + jnp.sum(other * other, axis=-1, keepdims=True)
    scale = lax.rsqrt(total / (2 * mine.shape[1]) + norm_eps)
    for index in range(mine.shape[1] // block):
        for held, side in ((mine, parity), (other, 1 - parity)):
            cols = pl.ds(pl.multiple_of((2 * index + side) * block, LANES), block)
            piece = held[:, index * block : (index + 1) * block]
            gain = gain_ref[layer_index : layer_index + 1, cols]
            normed_ref[:, cols] = (piece * scale * gain).astype(bf16)
    key_value_body(
        normed_ref[...], wk_ref[layer_index], wv_ref[layer_index],
        kg_ref[layer_index : layer_index + 1, :], kv_ref,
    )


def first_query_kernel(normed_ref, wq_hbm, qg_ref, q_ref, wq_ref, sems):
    share = wq_ref.shape[0] // sems.shape[0]
    copies = []
    for index in range(sems.shape[0]):
        at = pl.ds(index * share, share)
        copy = pltpu.make_async_copy(wq_hbm.at[0, at, :], wq_ref.at[at, :], sems.at[index])
        copy.start()
        copies.append(copy)
    flat = None
    for index, copy in enumerate(copies):
        copy.wait()
        at = slice(index * share, (index + 1) * share)
        piece = jnp.dot(normed_ref[:, at], wq_ref[at, :], preferred_element_type=f32)
        flat = piece if flat is None else flat + piece
    query_body(flat, qg_ref[0:1, :], q_ref)


def query_kernel(layer_index, normed_ref, wq_ref, qg_ref, q_ref):
    flat = jnp.dot(normed_ref[...], wq_ref[layer_index], preferred_element_type=f32)
    query_body(flat, qg_ref[layer_index : layer_index + 1, :], q_ref)


def query_body(flat, gain_row, q_ref):
    pieces = head_norm(flat, gain_row)
    width = pieces[0].shape[1]
    for index, piece in enumerate(pieces):
        scaled = piece.astype(bf16) * bf16(HEAD_DIM**-0.5)
        q_ref[:, index * width : (index + 1) * width] = scaled


def bias_kernel(layer_index, table_ref, tile_ref):
    heads, entries = table_ref.shape[1:]
    source = lax.broadcasted_iota(jnp.int32, (entries, LINE), 0)
    offset = lax.broadcasted_iota(jnp.int32, (entries, LINE), 1)
    distance = jnp.clip(WINDOW - 1 - offset, -CLIP, CLIP) + CLIP
    onehot = (source == distance).astype(f32)
    query_seg = lax.broadcasted_iota(jnp.int32, (CHUNK, WINDOW), 0) // SEG
    key_seg = lax.broadcasted_iota(jnp.int32, (CHUNK, WINDOW), 1) // SEG
    inside = (key_seg >= query_seg) & (key_seg <= query_seg + LEFT)
    line = jnp.dot(
        table_ref[layer_index], onehot, precision=lax.Precision.HIGHEST,
        preferred_element_type=f32,
    )
    for head in range(heads):
        spread = jnp.broadcast_to(line[head : head + 1, :], (CHUNK, LINE))
        rolled = pltpu.roll(spread, LINE - CHUNK + 1, 1, stride=1, stride_axis=0)
        tile_ref[head] = jnp.where(inside, rolled[:, :WINDOW], masked_score)


def attention_kernel(
    block, layer_index, q_start, starts, prior, place_ref, q_ref, *refs,
):
    piece_refs = refs[:PIECES]
    (
        tile_ref, wout_hbm, keep_ref, send_ref,
        keys_ref, even_ref, odd_ref, mixed_ref, wout_ref, sem,
    ) = refs[PIECES:]
    wout_copy = pltpu.make_async_copy(wout_hbm.at[layer_index], wout_ref, sem.at[0])
    wout_copy.start()
    first, parity = place_ref[0], place_ref[1]
    heads = q_ref.shape[1] // HEAD_DIM
    kv_width = piece_refs[0].shape[1] // 2
    kv_heads = kv_width // HEAD_DIM
    group = heads // kv_heads
    pairs = group // 2

    low = lax.broadcasted_iota(jnp.int32, (CHUNK, LANES), 1) < HEAD_DIM
    for index, piece_ref in enumerate(piece_refs):
        source = slice(starts[index], starts[index] + CHUNK)
        into = slice(index * CHUNK, (index + 1) * CHUNK)
        for kv in range(kv_heads):
            at = kv * HEAD_DIM
            key = piece_ref[source, at : at + HEAD_DIM].astype(f32)
            value = piece_ref[source, kv_width + at : kv_width + at + HEAD_DIM].astype(f32)
            key = jnp.concatenate([key, key], axis=1)
            value = jnp.concatenate([value, value], axis=1)
            keys_ref[kv, into, :] = key.astype(bf16)
            even_ref[kv, into, :] = jnp.where(low, value, 1.0).astype(bf16)
            odd_ref[kv, into, :] = jnp.where(low, 1.0, value).astype(bf16)

    key_index = lax.broadcasted_iota(jnp.int32, (1, WINDOW), 1)
    outside = jnp.where((key_index < prior * CHUNK) & (first == 1), masked_score, 0.0)
    for kv in range(kv_heads):
        evens, odds = [], []
        for pair in range(pairs):
            at = (kv * pairs + pair) * LANES
            both = q_ref[q_start : q_start + CHUNK, at : at + LANES]
            evens.append(jnp.where(low, both, jnp.zeros_like(both)))
            odds.append(jnp.where(low, jnp.zeros_like(both), both))
        stacked = jnp.concatenate(evens + odds, axis=0)
        scores = lax.dot_general(
            stacked, keys_ref[kv], (((1,), (1,)), ((), ())), preferred_element_type=f32
        )
        expons = []
        for index in range(group):
            pair, side = index % pairs, index // pairs
            head = kv * group + 2 * pair + side
            score = scores[index * CHUNK : (index + 1) * CHUNK, :] + tile_ref[head]
            if prior:
                score = score + outside
            peak = jnp.max(score, axis=-1, keepdims=True)
            expons.append(jnp.exp(score - peak).astype(bf16))
        even = jnp.dot(
            jnp.concatenate(expons[:pairs], axis=0), even_ref[kv], preferred_element_type=f32
        )
        odd = jnp.dot(
            jnp.concatenate(expons[pairs:], axis=0), odd_ref[kv], preferred_element_type=f32
        )
        for pair in range(pairs):
            at = (kv * pairs + pair) * LANES
            upper = even[pair * CHUNK : (pair + 1) * CHUNK, :]
            lower = odd[pair * CHUNK : (pair + 1) * CHUNK, :]
            total = pltpu.roll(jnp.where(low, lower, upper), HEAD_DIM, 1)
            mixed_ref[:, at : at + LANES] = (jnp.where(low, upper, lower) / total).astype(bf16)

    mixed = mixed_ref[...]
    wout_copy.wait()
    for index in range(keep_ref.shape[1] // block):
        for target, side in ((send_ref, 1 - parity), (keep_ref, parity)):
            cols = pl.ds(pl.multiple_of((2 * index + side) * block, LANES), block)
            partial_value = jnp.dot(mixed, wout_ref[:, cols], preferred_element_type=f32)
            target[:, index * block : (index + 1) * block] = partial_value.astype(bf16)


def add_kernel(a_ref, b_ref, out_ref):
    out_ref[...] = (a_ref[...].astype(f32) + b_ref[...].astype(f32)).astype(bf16)


def split_add_kernel(block, bit, place_ref, a_ref, b_ref, keep_ref, send_ref):
    parity = place_ref[bit]
    for index in range(keep_ref.shape[1] // block):
        into = slice(index * block, (index + 1) * block)
        for target, side in ((send_ref, 1 - parity), (keep_ref, parity)):
            cols = pl.ds(pl.multiple_of((2 * index + side) * block, LANES), block)
            target[:, into] = (
                a_ref[:, cols].astype(f32) + b_ref[:, cols].astype(f32)
            ).astype(bf16)


def residual_kernel(block, start, place_ref, x_ref, a_ref, b_ref, out_ref):
    rows = slice(start, start + out_ref.shape[0])
    for index in range(out_ref.shape[1] // block):
        into = slice(index * block, (index + 1) * block)
        cols = pl.ds(pl.multiple_of((2 * index + place_ref[1]) * block, LANES), block)
        added = a_ref[:, into].astype(f32) + b_ref[:, into].astype(f32)
        out_ref[:, into] = (x_ref[rows, cols].astype(f32) + added).astype(bf16)


def result_kernel(block, at, parts, place_ref, *refs):
    ins, out_hbm, held_ref, sems = refs[: 3 * parts], refs[-3], refs[-2], refs[-1]
    cols = pl.ds(pl.multiple_of(place_ref[at] * block, LANES), block)
    copies = []
    for part in range(parts):
        x_ref, a_ref, b_ref = ins[3 * part : 3 * part + 3]
        rows = slice(part * CHUNK, (part + 1) * CHUNK)
        added = a_ref[...].astype(f32) + b_ref[...].astype(f32)
        held_ref[rows, :] = (x_ref[:, cols].astype(f32) + added).astype(bf16)
        span = pl.ds(part * CHUNK, CHUNK)
        copy = pltpu.make_async_copy(held_ref.at[span, :], out_hbm.at[span, :], sems.at[part])
        copy.start()
        copies.append(copy)
    for copy in copies:
        copy.wait()


def swapped(value, bit):
    size = lax.axis_size("tp")
    return lax.ppermute(value, "tp", [(d, d ^ (1 << bit)) for d in range(size)])


def passed_along(value):
    return lax.ppermute(value, "sp", [(d, d + 1) for d in range(lax.axis_size("sp") - 1)])


def kept_in_hbm(*arrays):
    return [pltpu.with_memory_space_constraint(array, pltpu.HBM) for array in arrays]


def layers(stream, attn_gain, w_query, w_key, w_value, w_out, query_gain, key_gain, rel_bias):
    rows, width = stream.shape
    bits = lax.axis_size("tp").bit_length() - 1
    block = width // lax.axis_size("tp")
    half = width // 2
    query_width = w_query.shape[2]
    kv_width = w_key.shape[2]
    heads = query_width // HEAD_DIM
    kv_heads = kv_width // HEAD_DIM
    parts = rows // CHUNK
    order = list(reversed(range(parts)))
    tp_index = lax.axis_index("tp")
    place = jnp.stack(
        [(lax.axis_index("sp") == 0).astype(jnp.int32), tp_index % 2]
        + [(tp_index >> bit) & 1 for bit in range(1, bits)]
        + [tp_index // 2]
    ).astype(jnp.int32)

    def queries(layer_index, normed):
        count = normed.shape[0]
        return pl.pallas_call(
            functools.partial(query_kernel, layer_index),
            out_shape=out((count, query_width)),
            in_specs=[whole] * 3,
            out_specs=whole,
            compiler_params=params(),
            cost_estimate=cost(2 * count * width * query_width, 2 * width * query_width),
            name="queries",
        )(normed, w_query, query_gain)

    def attention(layer_index, part, query, q_start, pieces, starts):
        return pl.pallas_call(
            functools.partial(
                attention_kernel, block, layer_index, q_start, starts,
                max(0, PIECES - 1 - part),
            ),
            out_shape=[out((CHUNK, half))] * 2,
            in_specs=[scalar, whole] + [whole] * PIECES + [whole, in_hbm],
            out_specs=[whole, whole],
            scratch_shapes=[
                pltpu.VMEM((kv_heads, WINDOW, LANES), bf16),
                pltpu.VMEM((kv_heads, WINDOW, LANES), bf16),
                pltpu.VMEM((kv_heads, WINDOW, LANES), bf16),
                pltpu.VMEM((CHUNK, query_width), bf16),
                pltpu.VMEM((query_width, width), bf16),
                pltpu.SemaphoreType.DMA((1,)),
            ],
            compiler_params=params(),
            cost_estimate=cost(
                2 * CHUNK * query_width * (width + 4 * WINDOW), 2 * width * query_width
            ),
            name="attention",
        )(place, query, *pieces, tiles[layer_index], *kept_in_hbm(w_out))

    normed, kv = pl.pallas_call(
        first_norm_kernel,
        out_shape=[out((rows, width)), out((rows, 2 * kv_width))],
        in_specs=[in_hbm] * 5,
        out_specs=[whole, whole],
        scratch_shapes=[
            pltpu.VMEM(stream.shape, bf16),
            pltpu.VMEM(attn_gain.shape, f32),
            pltpu.VMEM((width, kv_width), bf16),
            pltpu.VMEM((width, kv_width), bf16),
            pltpu.VMEM(key_gain.shape, f32),
            pltpu.SemaphoreType.DMA((4,)),
            pltpu.SemaphoreType.DMA((4,)),
        ],
        compiler_params=params(),
        cost_estimate=cost(4 * rows * width * kv_width, 4 * rows * width),
        name="norm_kv_first",
    )(*kept_in_hbm(stream, attn_gain, w_key, w_value, key_gain))
    kv_prior = passed_along(kv[rows - REACH :])
    query = pl.pallas_call(
        first_query_kernel,
        out_shape=out((rows, query_width)),
        in_specs=[whole, in_hbm, whole],
        out_specs=whole,
        scratch_shapes=[
            pltpu.VMEM((width, query_width), bf16),
            pltpu.SemaphoreType.DMA((4,)),
        ],
        compiler_params=params(),
        cost_estimate=cost(2 * rows * width * query_width, 2 * width * query_width),
        name="queries",
    )(normed, *kept_in_hbm(w_query), query_gain)
    tiles = []
    for layer_index in range(LAYERS):
        tiles.append(
            pl.pallas_call(
                functools.partial(bias_kernel, layer_index),
                out_shape=out((heads, CHUNK, WINDOW), f32),
                in_specs=[whole],
                out_specs=whole,
                compiler_params=params(),
                cost_estimate=cost(5e8, 1e6),
                name="bias_tiles",
            )(rel_bias)
        )

    mine, other, kvs, normeds = {}, {}, {}, {}
    for part in order:
        pieces, starts = [], []
        for index in range(PIECES):
            behind = part - (PIECES - 1) + index
            pieces.append(kv_prior if behind < 0 else kv)
            starts.append((behind + PIECES - 1 if behind < 0 else behind) * CHUNK)
        keep, send = attention(0, part, query, part * CHUNK, pieces, starts)
        received = swapped(send, 0)
        for bit in range(1, bits):
            summed = pl.pallas_call(
                add_kernel,
                out_shape=out((CHUNK, half)),
                in_specs=[whole, whole],
                out_specs=whole,
                compiler_params=params(),
                name="add",
            )(keep, received)
            keep, received = summed, swapped(summed, bit)
        mine[part] = pl.pallas_call(
            functools.partial(residual_kernel, block, part * CHUNK),
            out_shape=out((CHUNK, half)),
            in_specs=[scalar, whole, whole, whole],
            out_specs=whole,
            compiler_params=params(),
            name="residual",
        )(place, stream, keep, received)
        other[part] = swapped(mine[part], 0)

    priors = {}
    for part in order:
        normeds[part], kvs[part] = pl.pallas_call(
            functools.partial(next_norm_kernel, 1, block),
            out_shape=[out((CHUNK, width)), out((CHUNK, 2 * kv_width))],
            in_specs=[scalar] + [whole] * 6,
            out_specs=[whole, whole],
            compiler_params=params(),
            cost_estimate=cost(4 * CHUNK * width * kv_width, 4 * CHUNK * width),
            name="norm_kv_next",
        )(place, mine[part], other[part], attn_gain, w_key, w_value, key_gain)
        if part >= parts - (PIECES - 1):
            priors[part - parts] = passed_along(kvs[part])

    outs = {}
    for part in order:
        query = queries(1, normeds[part])
        pieces = []
        for index in range(PIECES):
            behind = part - (PIECES - 1) + index
            pieces.append(priors[behind] if behind < 0 else kvs[behind])
        keep, send = attention(1, part, query, 0, pieces, [0] * PIECES)
        received = swapped(send, 0)
        for bit in range(1, bits):
            left = keep.shape[1] // 2
            keep, send = pl.pallas_call(
                functools.partial(split_add_kernel, block, 1 + bit),
                out_shape=[out((CHUNK, left))] * 2,
                in_specs=[scalar, whole, whole],
                out_specs=[whole, whole],
                compiler_params=params(),
                name="split_add",
            )(place, keep, received)
            received = swapped(send, bit)
        outs[part] = (mine[part], keep, received)

    return pl.pallas_call(
        functools.partial(result_kernel, block, bits + 1, parts),
        out_shape=out((rows, block)),
        in_specs=[scalar] + [whole] * (3 * parts),
        out_specs=in_hbm,
        scratch_shapes=[
            pltpu.VMEM((rows, block), bf16),
            pltpu.SemaphoreType.DMA((parts,)),
        ],
        compiler_params=params(),
        name="result",
    )(place, *[ref for part in range(parts) for ref in outs[part]])


def solution(mesh):
    return jax.shard_map(
        layers,
        mesh=mesh,
        in_specs=(
            P("sp", None),
            P(),
            P(None, None, "tp"),
            P(None, None, "tp"),
            P(None, None, "tp"),
            P(None, "tp", None),
            P(),
            P(),
            P(None, "tp", None),
        ),
        out_specs=P("sp", "tp"),
        check_vma=False,
    )
```

```python
import functools

import jax
import jax.numpy as jnp
from jax import lax
from jax.experimental import pallas as pl
from jax.experimental.pallas import tpu as pltpu
from jax.sharding import PartitionSpec as P


HEAD_DIM = 64
SEG = 64
LEFT = 4
CLIP = 128
LAYERS = 2

REACH = LEFT * SEG
CHUNK = 2 * SEG
PIECES = REACH // CHUNK + 1
WINDOW = REACH + CHUNK
LINE = WINDOW + CHUNK
LANES = 128

norm_eps = 1e-06
masked_score = -1e30

bf16 = jnp.bfloat16
f32 = jnp.float32

whole = pl.BlockSpec(memory_space=pltpu.VMEM)
in_hbm = pl.BlockSpec(memory_space=pltpu.HBM)


def params():
    return pltpu.CompilerParams(vmem_limit_bytes=12 * 1024 * 1024)


def cost(flops, moved):
    return pl.CostEstimate(flops=int(flops), bytes_accessed=int(moved), transcendentals=0)


def out(shape, dtype=bf16):
    return jax.ShapeDtypeStruct(shape, dtype)


def head_norm(flat, gain_row):
    width = flat.shape[1]
    step = min(width, LANES)
    row = lax.broadcasted_iota(jnp.int32, (step, step), 0) // HEAD_DIM
    col = lax.broadcasted_iota(jnp.int32, (step, step), 1) // HEAD_DIM
    mean_of = jnp.where(row == col, 1.0 / HEAD_DIM, 0.0).astype(bf16)
    gain = jnp.concatenate([gain_row] * (step // HEAD_DIM), axis=1)
    pieces = []
    for lower in range(0, width, step):
        part = flat[:, lower : lower + step]
        squared = part * part
        high = squared.astype(bf16)
        low = (squared - high.astype(f32)).astype(bf16)
        mean = jnp.dot(high, mean_of, preferred_element_type=f32) + jnp.dot(
            low, mean_of, preferred_element_type=f32
        )
        pieces.append(part * lax.rsqrt(mean + norm_eps) * gain)
    return pieces


def key_value_body(normed, wk, wv, key_gain_row, kv_ref):
    keys = jnp.dot(normed, wk, preferred_element_type=f32)
    values = jnp.dot(normed, wv, preferred_element_type=f32)
    keys = head_norm(keys, key_gain_row)[0]
    kv_ref[...] = jnp.concatenate([keys, values], axis=1).astype(bf16)


def first_norm_kernel(
    x_hbm, gain_hbm, wk_hbm, wv_hbm, kg_hbm, table_hbm, normed_ref, kv_ref, table_ref,
    x_ref, gain_ref, wk_ref, wv_ref, kg_ref, row_sems, sems,
):
    steps = row_sems.shape[0]
    share = x_ref.shape[0] // steps
    row_copies = []
    for index in range(steps):
        at = pl.ds(index * share, share)
        row_copies.append(
            pltpu.make_async_copy(x_hbm.at[at, :], x_ref.at[at, :], row_sems.at[index])
        )
    gain_copy = pltpu.make_async_copy(gain_hbm, gain_ref, sems.at[0])
    late = [
        pltpu.make_async_copy(wk_hbm.at[0], wk_ref, sems.at[1]),
        pltpu.make_async_copy(wv_hbm.at[0], wv_ref, sems.at[2]),
        pltpu.make_async_copy(kg_hbm, kg_ref, sems.at[3]),
        pltpu.make_async_copy(table_hbm, table_ref, sems.at[4]),
    ]
    for copy in [gain_copy] + row_copies + late:
        copy.start()
    gain_copy.wait()
    gain = gain_ref[0:1, :]
    for index, copy in enumerate(row_copies):
        copy.wait()
        at = slice(index * share, (index + 1) * share)
        current = x_ref[at, :].astype(f32)
        mean = jnp.mean(current * current, axis=-1, keepdims=True)
        normed_ref[at, :] = (current * lax.rsqrt(mean + norm_eps) * gain).astype(bf16)
    for copy in late:
        copy.wait()
    key_value_body(normed_ref[...], wk_ref[...], wv_ref[...], kg_ref[0:1, :], kv_ref)


def next_norm_kernel(
    layer_index, block, mine_ref, other_ref, gain_ref, wk_ref, wv_ref, kg_ref,
    normed_ref, kv_ref,
):
    parity = lax.axis_index("tp") % 2
    mine = mine_ref[...].astype(f32)
    other = other_ref[...].astype(f32)
    total = jnp.sum(mine * mine, axis=-1, keepdims=True)
    total = total + jnp.sum(other * other, axis=-1, keepdims=True)
    scale = lax.rsqrt(total / (2 * mine.shape[1]) + norm_eps)
    for index in range(mine.shape[1] // block):
        for held, side in ((mine, parity), (other, 1 - parity)):
            cols = pl.ds(pl.multiple_of((2 * index + side) * block, LANES), block)
            piece = held[:, index * block : (index + 1) * block]
            gain = gain_ref[layer_index : layer_index + 1, cols]
            normed_ref[:, cols] = (piece * scale * gain).astype(bf16)
    key_value_body(
        normed_ref[...], wk_ref[layer_index], wv_ref[layer_index],
        kg_ref[layer_index : layer_index + 1, :], kv_ref,
    )


def query_kernel(layer_index, normed_ref, wq_ref, qg_ref, q_ref):
    flat = jnp.dot(normed_ref[...], wq_ref[layer_index], preferred_element_type=f32)
    query_body(flat, qg_ref[layer_index : layer_index + 1, :], q_ref)


def query_body(flat, gain_row, q_ref):
    pieces = head_norm(flat, gain_row)
    width = pieces[0].shape[1]
    for index, piece in enumerate(pieces):
        scaled = piece.astype(bf16) * bf16(HEAD_DIM**-0.5)
        q_ref[:, index * width : (index + 1) * width] = scaled


def bias_kernel(layer_index, table_ref, tile_ref):
    heads, entries = table_ref.shape[1:]
    source = lax.broadcasted_iota(jnp.int32, (entries, LINE), 0)
    offset = lax.broadcasted_iota(jnp.int32, (entries, LINE), 1)
    distance = jnp.clip(WINDOW - 1 - offset, -CLIP, CLIP) + CLIP
    onehot = (source == distance).astype(f32)
    query_seg = lax.broadcasted_iota(jnp.int32, (CHUNK, WINDOW), 0) // SEG
    key_seg = lax.broadcasted_iota(jnp.int32, (CHUNK, WINDOW), 1) // SEG
    inside = (key_seg >= query_seg) & (key_seg <= query_seg + LEFT)
    line = jnp.dot(
        table_ref[layer_index], onehot, precision=lax.Precision.HIGHEST,
        preferred_element_type=f32,
    )
    for head in range(heads):
        spread = jnp.broadcast_to(line[head : head + 1, :], (CHUNK, LINE))
        rolled = pltpu.roll(spread, LINE - CHUNK + 1, 1, stride=1, stride_axis=0)
        tile_ref[head] = jnp.where(inside, rolled[:, :WINDOW], masked_score)


def attention_kernel(
    block, layer_index, q_start, starts, prior, q_ref, *refs,
):
    piece_refs = refs[:PIECES]
    (
        tile_ref, wout_ref, keep_ref, send_ref,
        keys_ref, even_ref, odd_ref, mixed_ref,
    ) = refs[PIECES:]
    parity = lax.axis_index("tp") % 2
    heads = q_ref.shape[1] // HEAD_DIM
    kv_width = piece_refs[0].shape[1] // 2
    kv_heads = kv_width // HEAD_DIM
    group = heads // kv_heads
    pairs = group // 2

    low = lax.broadcasted_iota(jnp.int32, (CHUNK, LANES), 1) < HEAD_DIM
    for index, piece_ref in enumerate(piece_refs):
        source = slice(starts[index], starts[index] + CHUNK)
        into = slice(index * CHUNK, (index + 1) * CHUNK)
        for kv in range(kv_heads):
            at = kv * HEAD_DIM
            key = piece_ref[source, at : at + HEAD_DIM].astype(f32)
            value = piece_ref[source, kv_width + at : kv_width + at + HEAD_DIM].astype(f32)
            key = jnp.concatenate([key, key], axis=1)
            value = jnp.concatenate([value, value], axis=1)
            keys_ref[kv, into, :] = key.astype(bf16)
            even_ref[kv, into, :] = jnp.where(low, value, 1.0).astype(bf16)
            odd_ref[kv, into, :] = jnp.where(low, 1.0, value).astype(bf16)

    key_index = lax.broadcasted_iota(jnp.int32, (1, WINDOW), 1)
    outside = jnp.where((key_index < prior * CHUNK) & (lax.axis_index("sp") == 0), masked_score, 0.0)
    for kv in range(kv_heads):
        evens, odds = [], []
        for pair in range(pairs):
            at = (kv * pairs + pair) * LANES
            both = q_ref[q_start : q_start + CHUNK, at : at + LANES]
            evens.append(jnp.where(low, both, jnp.zeros_like(both)))
            odds.append(jnp.where(low, jnp.zeros_like(both), both))
        stacked = jnp.concatenate(evens + odds, axis=0)
        scores = lax.dot_general(
            stacked, keys_ref[kv], (((1,), (1,)), ((), ())), preferred_element_type=f32
        )
        expons = []
        for index in range(group):
            pair, side = index % pairs, index // pairs
            head = kv * group + 2 * pair + side
            score = scores[index * CHUNK : (index + 1) * CHUNK, :] + tile_ref[head]
            if prior:
                score = score + outside
            peak = jnp.max(score, axis=-1, keepdims=True)
            expons.append(jnp.exp(score - peak).astype(bf16))
        even = jnp.dot(
            jnp.concatenate(expons[:pairs], axis=0), even_ref[kv], preferred_element_type=f32
        )
        odd = jnp.dot(
            jnp.concatenate(expons[pairs:], axis=0), odd_ref[kv], preferred_element_type=f32
        )
        for pair in range(pairs):
            at = (kv * pairs + pair) * LANES
            upper = even[pair * CHUNK : (pair + 1) * CHUNK, :]
            lower = odd[pair * CHUNK : (pair + 1) * CHUNK, :]
            total = pltpu.roll(jnp.where(low, lower, upper), HEAD_DIM, 1)
            mixed_ref[:, at : at + LANES] = (jnp.where(low, upper, lower) / total).astype(bf16)

    mixed = mixed_ref[...]
    for index in range(keep_ref.shape[1] // block):
        for target, side in ((send_ref, 1 - parity), (keep_ref, parity)):
            cols = pl.ds(pl.multiple_of((2 * index + side) * block, LANES), block)
            partial_value = jnp.dot(mixed, wout_ref[layer_index, :, cols], preferred_element_type=f32)
            target[:, index * block : (index + 1) * block] = partial_value.astype(bf16)


def add_kernel(a_ref, b_ref, out_ref):
    out_ref[...] = (a_ref[...].astype(f32) + b_ref[...].astype(f32)).astype(bf16)


def split_add_kernel(block, bit, a_ref, b_ref, keep_ref, send_ref):
    parity = (lax.axis_index("tp") >> bit) & 1
    for index in range(keep_ref.shape[1] // block):
        into = slice(index * block, (index + 1) * block)
        for target, side in ((send_ref, 1 - parity), (keep_ref, parity)):
            cols = pl.ds(pl.multiple_of((2 * index + side) * block, LANES), block)
            target[:, into] = (
                a_ref[:, cols].astype(f32) + b_ref[:, cols].astype(f32)
            ).astype(bf16)


def residual_kernel(block, start, x_ref, a_ref, b_ref, out_ref):
    rows = slice(start, start + out_ref.shape[0])
    parity = lax.axis_index("tp") % 2
    for index in range(out_ref.shape[1] // block):
        into = slice(index * block, (index + 1) * block)
        cols = pl.ds(pl.multiple_of((2 * index + parity) * block, LANES), block)
        added = a_ref[:, into].astype(f32) + b_ref[:, into].astype(f32)
        out_ref[:, into] = (x_ref[rows, cols].astype(f32) + added).astype(bf16)


def result_kernel(block, parts, *refs):
    ins, out_hbm, held_ref, sems = refs[: 3 * parts], refs[-3], refs[-2], refs[-1]
    cols = pl.ds(pl.multiple_of((lax.axis_index("tp") // 2) * block, LANES), block)
    copies = []
    for part in range(parts):
        x_ref, a_ref, b_ref = ins[3 * part : 3 * part + 3]
        rows = slice(part * CHUNK, (part + 1) * CHUNK)
        added = a_ref[...].astype(f32) + b_ref[...].astype(f32)
        held_ref[rows, :] = (x_ref[:, cols].astype(f32) + added).astype(bf16)
        span = pl.ds(part * CHUNK, CHUNK)
        copy = pltpu.make_async_copy(held_ref.at[span, :], out_hbm.at[span, :], sems.at[part])
        copy.start()
        copies.append(copy)
    for copy in copies:
        copy.wait()


def swapped(value, bit):
    size = lax.axis_size("tp")
    return lax.ppermute(value, "tp", [(d, d ^ (1 << bit)) for d in range(size)])


def passed_along(value):
    return lax.ppermute(value, "sp", [(d, d + 1) for d in range(lax.axis_size("sp") - 1)])


def kept_in_hbm(*arrays):
    return [pltpu.with_memory_space_constraint(array, pltpu.HBM) for array in arrays]


def layers(stream, attn_gain, w_query, w_key, w_value, w_out, query_gain, key_gain, rel_bias):
    rows, width = stream.shape
    bits = lax.axis_size("tp").bit_length() - 1
    block = width // lax.axis_size("tp")
    half = width // 2
    query_width = w_query.shape[2]
    kv_width = w_key.shape[2]
    heads = query_width // HEAD_DIM
    kv_heads = kv_width // HEAD_DIM
    parts = rows // CHUNK
    order = list(reversed(range(parts)))

    def queries(layer_index, normed):
        count = normed.shape[0]
        return pl.pallas_call(
            functools.partial(query_kernel, layer_index),
            out_shape=out((count, query_width)),
            in_specs=[whole] * 3,
            out_specs=whole,
            compiler_params=params(),
            cost_estimate=cost(2e9, 2 * width * query_width),
            name="queries",
        )(normed, w_query, query_gain)

    def attention(layer_index, part, query, q_start, pieces, starts):
        return pl.pallas_call(
            functools.partial(
                attention_kernel, block, layer_index, q_start, starts,
                max(0, PIECES - 1 - part),
            ),
            out_shape=[out((CHUNK, half))] * 2,
            in_specs=[whole] * (PIECES + 3),
            out_specs=[whole, whole],
            scratch_shapes=[
                pltpu.VMEM((kv_heads, WINDOW, LANES), bf16),
                pltpu.VMEM((kv_heads, WINDOW, LANES), bf16),
                pltpu.VMEM((kv_heads, WINDOW, LANES), bf16),
                pltpu.VMEM((CHUNK, query_width), bf16),
            ],
            compiler_params=params(),
            cost_estimate=cost(
                2 * CHUNK * query_width * (width + 4 * WINDOW), 2 * width * query_width
            ),
            name="attention",
        )(query, *pieces, tiles[layer_index], w_out)

    normed, kv, table = pl.pallas_call(
        first_norm_kernel,
        out_shape=[
            out((rows, width)), out((rows, 2 * kv_width)), out(rel_bias.shape, f32)
        ],
        in_specs=[in_hbm] * 6,
        out_specs=[whole] * 3,
        scratch_shapes=[
            pltpu.VMEM(stream.shape, bf16),
            pltpu.VMEM(attn_gain.shape, f32),
            pltpu.VMEM((width, kv_width), bf16),
            pltpu.VMEM((width, kv_width), bf16),
            pltpu.VMEM(key_gain.shape, f32),
            pltpu.SemaphoreType.DMA((4,)),
            pltpu.SemaphoreType.DMA((5,)),
        ],
        compiler_params=params(),
        cost_estimate=cost(3e9, 4 * rows * width),
        name="norm_kv_first",
    )(*kept_in_hbm(stream, attn_gain, w_key, w_value, key_gain, rel_bias))
    kv_prior = passed_along(kv[rows - REACH :])
    query = queries(0, normed)
    tiles = []
    for layer_index in range(LAYERS):
        tiles.append(
            pl.pallas_call(
                functools.partial(bias_kernel, layer_index),
                out_shape=out((heads, CHUNK, WINDOW), f32),
                in_specs=[whole],
                out_specs=whole,
                compiler_params=params(),
                cost_estimate=cost(2e9, 1e6),
                name="bias_tiles",
            )(table)
        )

    mine, other, kvs, normeds = {}, {}, {}, {}
    for part in order:
        pieces, starts = [], []
        for index in range(PIECES):
            behind = part - (PIECES - 1) + index
            pieces.append(kv_prior if behind < 0 else kv)
            starts.append((behind + PIECES - 1 if behind < 0 else behind) * CHUNK)
        keep, send = attention(0, part, query, part * CHUNK, pieces, starts)
        received = swapped(send, 0)
        for bit in range(1, bits):
            summed = pl.pallas_call(
                add_kernel,
                out_shape=out((CHUNK, half)),
                in_specs=[whole, whole],
                out_specs=whole,
                compiler_params=params(),
                name="add",
            )(keep, received)
            keep, received = summed, swapped(summed, bit)
        mine[part] = pl.pallas_call(
            functools.partial(residual_kernel, block, part * CHUNK),
            out_shape=out((CHUNK, half)),
            in_specs=[whole, whole, whole],
            out_specs=whole,
            compiler_params=params(),
            name="residual",
        )(stream, keep, received)
        other[part] = swapped(mine[part], 0)

    priors = {}
    for part in order:
        normeds[part], kvs[part] = pl.pallas_call(
            functools.partial(next_norm_kernel, 1, block),
            out_shape=[out((CHUNK, width)), out((CHUNK, 2 * kv_width))],
            in_specs=[whole] * 6,
            out_specs=[whole, whole],
            compiler_params=params(),
            cost_estimate=cost(4 * CHUNK * width * kv_width, 4 * CHUNK * width),
            name="norm_kv_next",
        )(mine[part], other[part], attn_gain, w_key, w_value, key_gain)
        if part >= parts - (PIECES - 1):
            priors[part - parts] = passed_along(kvs[part])

    outs = {}
    for part in order:
        query = queries(1, normeds[part])
        pieces = []
        for index in range(PIECES):
            behind = part - (PIECES - 1) + index
            pieces.append(priors[behind] if behind < 0 else kvs[behind])
        keep, send = attention(1, part, query, 0, pieces, [0] * PIECES)
        received = swapped(send, 0)
        for bit in range(1, bits):
            left = keep.shape[1] // 2
            keep, send = pl.pallas_call(
                functools.partial(split_add_kernel, block, bit),
                out_shape=[out((CHUNK, left))] * 2,
                in_specs=[whole, whole],
                out_specs=[whole, whole],
                compiler_params=params(),
                name="split_add",
            )(keep, received)
            received = swapped(send, bit)
        outs[part] = (mine[part], keep, received)

    return pl.pallas_call(
        functools.partial(result_kernel, block, parts),
        out_shape=out((rows, block)),
        in_specs=[whole] * (3 * parts),
        out_specs=in_hbm,
        scratch_shapes=[
            pltpu.VMEM((rows, block), bf16),
            pltpu.SemaphoreType.DMA((parts,)),
        ],
        compiler_params=params(),
        name="result",
    )(*[ref for part in range(parts) for ref in outs[part]])


def solution(mesh):
    return jax.shard_map(
        layers,
        mesh=mesh,
        in_specs=(
            P("sp", None),
            P(),
            P(None, None, "tp"),
            P(None, None, "tp"),
            P(None, None, "tp"),
            P(None, "tp", None),
            P(),
            P(),
            P(None, "tp", None),
        ),
        out_specs=P("sp", "tp"),
        check_vma=False,
    )
```

```python
import functools

import jax
import jax.numpy as jnp
from jax import lax
from jax.experimental import pallas as pl
from jax.experimental.pallas import tpu as pltpu
from jax.sharding import PartitionSpec as P


HEAD_DIM = 64
SEG = 64
LEFT = 4
CLIP = 128
LAYERS = 2

REACH = LEFT * SEG
CHUNK = 2 * SEG
PIECES = REACH // CHUNK + 1
WINDOW = REACH + CHUNK
LINE = WINDOW + CHUNK
LANES = 128

norm_eps = 1e-06
masked_score = -1e30

LOG2_E = 1.4426950408889634

bf16 = jnp.bfloat16
f32 = jnp.float32

whole = pl.BlockSpec(memory_space=pltpu.VMEM)
in_hbm = pl.BlockSpec(memory_space=pltpu.HBM)


def params():
    return pltpu.CompilerParams(vmem_limit_bytes=12 * 1024 * 1024)


def cost(flops, moved):
    return pl.CostEstimate(flops=int(flops), bytes_accessed=int(moved), transcendentals=0)


def out(shape, dtype=bf16):
    return jax.ShapeDtypeStruct(shape, dtype)


def head_norm(flat, gain_row):
    width = flat.shape[1]
    step = min(width, LANES)
    row = lax.broadcasted_iota(jnp.int32, (step, step), 0) // HEAD_DIM
    col = lax.broadcasted_iota(jnp.int32, (step, step), 1) // HEAD_DIM
    mean_of = jnp.where(row == col, 1.0 / HEAD_DIM, 0.0).astype(bf16)
    gain = jnp.concatenate([gain_row] * (step // HEAD_DIM), axis=1)
    pieces = []
    for lower in range(0, width, step):
        part = flat[:, lower : lower + step]
        squared = part * part
        high = squared.astype(bf16)
        low = (squared - high.astype(f32)).astype(bf16)
        mean = jnp.dot(high, mean_of, preferred_element_type=f32) + jnp.dot(
            low, mean_of, preferred_element_type=f32
        )
        pieces.append(part * lax.rsqrt(mean + norm_eps) * gain)
    return pieces


def key_value_body(normed, wk, wv, key_gain_row, kv_ref):
    keys = jnp.dot(normed, wk, preferred_element_type=f32)
    values = jnp.dot(normed, wv, preferred_element_type=f32)
    keys = head_norm(keys, key_gain_row)[0]
    kv_ref[...] = jnp.concatenate([keys, values], axis=1).astype(bf16)


def first_norm_kernel(
    x_hbm, gain_hbm, wk_hbm, wv_hbm, kg_hbm, table_hbm, normed_ref, kv_ref, table_ref,
    x_ref, gain_ref, wk_ref, wv_ref, kg_ref, row_sems, sems,
):
    steps = row_sems.shape[0]
    share = x_ref.shape[0] // steps
    row_copies = []
    for index in range(steps):
        at = pl.ds(index * share, share)
        row_copies.append(
            pltpu.make_async_copy(x_hbm.at[at, :], x_ref.at[at, :], row_sems.at[index])
        )
    gain_copy = pltpu.make_async_copy(gain_hbm, gain_ref, sems.at[0])
    late = [
        pltpu.make_async_copy(wk_hbm.at[0], wk_ref, sems.at[1]),
        pltpu.make_async_copy(wv_hbm.at[0], wv_ref, sems.at[2]),
        pltpu.make_async_copy(kg_hbm, kg_ref, sems.at[3]),
        pltpu.make_async_copy(table_hbm, table_ref, sems.at[4]),
    ]
    for copy in [gain_copy] + row_copies + late:
        copy.start()
    gain_copy.wait()
    gain = gain_ref[0:1, :]
    for index, copy in enumerate(row_copies):
        copy.wait()
        at = slice(index * share, (index + 1) * share)
        current = x_ref[at, :].astype(f32)
        mean = jnp.mean(current * current, axis=-1, keepdims=True)
        normed_ref[at, :] = (current * lax.rsqrt(mean + norm_eps) * gain).astype(bf16)
    for copy in late:
        copy.wait()
    key_value_body(normed_ref[...], wk_ref[...], wv_ref[...], kg_ref[0:1, :], kv_ref)


def next_norm_kernel(
    layer_index, block, mine_ref, other_ref, gain_ref, wk_ref, wv_ref, kg_ref,
    normed_ref, kv_ref,
):
    parity = lax.axis_index("tp") % 2
    mine = mine_ref[...].astype(f32)
    other = other_ref[...].astype(f32)
    total = jnp.sum(mine * mine, axis=-1, keepdims=True)
    total = total + jnp.sum(other * other, axis=-1, keepdims=True)
    scale = lax.rsqrt(total / (2 * mine.shape[1]) + norm_eps)
    for index in range(mine.shape[1] // block):
        for held, side in ((mine, parity), (other, 1 - parity)):
            cols = pl.ds(pl.multiple_of((2 * index + side) * block, LANES), block)
            piece = held[:, index * block : (index + 1) * block]
            gain = gain_ref[layer_index : layer_index + 1, cols]
            normed_ref[:, cols] = (piece * scale * gain).astype(bf16)
    key_value_body(
        normed_ref[...], wk_ref[layer_index], wv_ref[layer_index],
        kg_ref[layer_index : layer_index + 1, :], kv_ref,
    )


def query_kernel(layer_index, normed_ref, wq_ref, qg_ref, q_ref):
    flat = jnp.dot(normed_ref[...], wq_ref[layer_index], preferred_element_type=f32)
    query_body(flat, qg_ref[layer_index : layer_index + 1, :], q_ref)


def query_body(flat, gain_row, q_ref):
    pieces = head_norm(flat, gain_row * (HEAD_DIM**-0.5 * LOG2_E))
    kv_width = q_ref.shape[2]
    group = q_ref.shape[0] * HEAD_DIM // kv_width
    lanes = pieces[0].shape[1]
    for head in range(q_ref.shape[0]):
        at = head * HEAD_DIM
        piece = pieces[at // lanes][:, at % lanes : at % lanes + HEAD_DIM]
        before = head // group * HEAD_DIM
        after = kv_width - HEAD_DIM - before
        rows = piece.shape[0]
        spread = [jnp.zeros((rows, before), f32)] if before else []
        spread += [piece] + ([jnp.zeros((rows, after), f32)] if after else [])
        q_ref[head] = jnp.concatenate(spread, axis=1).astype(bf16)


def bias_kernel(layer_index, table_ref, tile_ref):
    heads, entries = table_ref.shape[1:]
    source = lax.broadcasted_iota(jnp.int32, (entries, LINE), 0)
    offset = lax.broadcasted_iota(jnp.int32, (entries, LINE), 1)
    distance = jnp.clip(WINDOW - 1 - offset, -CLIP, CLIP) + CLIP
    onehot = (source == distance).astype(f32)
    query_seg = lax.broadcasted_iota(jnp.int32, (CHUNK, WINDOW), 0) // SEG
    key_seg = lax.broadcasted_iota(jnp.int32, (CHUNK, WINDOW), 1) // SEG
    inside = (key_seg >= query_seg) & (key_seg <= query_seg + LEFT)
    line = jnp.dot(
        table_ref[layer_index] * LOG2_E, onehot, precision=lax.Precision.HIGHEST,
        preferred_element_type=f32,
    )
    for head in range(heads):
        spread = jnp.broadcast_to(line[head : head + 1, :], (CHUNK, LINE))
        rolled = pltpu.roll(spread, LINE - CHUNK + 1, 1, stride=1, stride_axis=0)
        tile_ref[head] = jnp.where(inside, rolled[:, :WINDOW], masked_score)


def attention_kernel(
    block, layer_index, q_start, row_start, step, starts, prior, q_ref, *refs,
):
    piece_refs = refs[:PIECES]
    tile_ref, wout_ref, keep_ref, send_ref, mixed_ref = refs[PIECES:]
    heads = q_ref.shape[0]
    kv_width = q_ref.shape[2]
    group = heads * HEAD_DIM // kv_width
    count = keep_ref.shape[0]
    rows = slice(q_start, q_start + count)

    pieces = [
        ref[start : start + CHUNK, :] for ref, start in zip(piece_refs, starts, strict=True)
    ]
    keys = jnp.concatenate([piece[:, :kv_width] for piece in pieces], axis=0)
    values = jnp.concatenate([piece[:, kv_width:] for piece in pieces], axis=0)
    values = jnp.concatenate([values, jnp.ones_like(values)], axis=1)
    key_index = lax.broadcasted_iota(jnp.int32, (1, WINDOW), 1)
    outside = (key_index < prior * CHUNK) & (lax.axis_index("sp") == 0)
    outside = jnp.where(outside, masked_score, 0.0)
    for first in range(0, heads, step):
        stacked = jnp.concatenate([q_ref[first + index, rows, :] for index in range(step)], axis=0)
        scores = lax.dot_general(
            stacked, keys, (((1,), (1,)), ((), ())), preferred_element_type=f32
        )
        expons = []
        for index in range(step):
            score = scores[index * count : (index + 1) * count, :]
            score = score + tile_ref[first + index, row_start : row_start + count, :]
            if prior:
                score = score + outside
            peak = jnp.max(score, axis=-1, keepdims=True)
            expons.append(jnp.exp2(score - peak).astype(bf16))
        summed = jnp.dot(
            jnp.concatenate(expons, axis=0), values, preferred_element_type=f32
        )
        ratio = summed[:, :kv_width] / summed[:, kv_width:]
        for index in range(step):
            at = (first + index) // group * HEAD_DIM
            into = (first + index) * HEAD_DIM
            part = ratio[index * count : (index + 1) * count, at : at + HEAD_DIM]
            mixed_ref[:, into : into + HEAD_DIM] = part.astype(bf16)

    out_projection(block, layer_index, mixed_ref, wout_ref, keep_ref, send_ref)


def out_projection(block, layer_index, mixed_ref, wout_ref, keep_ref, send_ref):
    parity = lax.axis_index("tp") % 2
    mixed = mixed_ref[...]
    for index in range(keep_ref.shape[1] // block):
        for target, side in ((send_ref, 1 - parity), (keep_ref, parity)):
            cols = pl.ds(pl.multiple_of((2 * index + side) * block, LANES), block)
            partial_value = jnp.dot(
                mixed, wout_ref[layer_index, :, cols], preferred_element_type=f32
            )
            target[:, index * block : (index + 1) * block] = partial_value.astype(bf16)


def own_kernel(q_start, starts, q_ref, *refs):
    piece_refs = refs[: len(starts)]
    tile_ref, peak_ref, summed_ref = refs[len(starts) :]
    kv_width = q_ref.shape[2]
    rows = slice(q_start, q_start + CHUNK)
    pieces = [
        ref[start : start + CHUNK, :] for ref, start in zip(piece_refs, starts, strict=True)
    ]
    keys = jnp.concatenate([piece[:, :kv_width] for piece in pieces], axis=0)
    values = jnp.concatenate([piece[:, kv_width:] for piece in pieces], axis=0)
    values = jnp.concatenate([values, jnp.ones_like(values)], axis=1)
    lower = WINDOW - len(starts) * CHUNK
    heads = q_ref.shape[0]
    scores = lax.dot_general(
        q_ref[:, rows, :].reshape(heads * CHUNK, kv_width), keys, (((1,), (1,)), ((), ())),
        preferred_element_type=f32,
    ).reshape(heads, CHUNK, keys.shape[0])
    scores = scores + tile_ref[:, :, lower:]
    peaks = jnp.max(scores, axis=-1, keepdims=True)
    expons = jnp.exp2(scores - peaks).astype(bf16)
    peak_ref[...] = jnp.broadcast_to(peaks, peak_ref.shape)
    summed = jnp.dot(
        expons.reshape(heads * CHUNK, keys.shape[0]), values, preferred_element_type=f32
    )
    summed_ref[...] = summed.reshape(summed_ref.shape)


def joined_kernel(block, layer_index, q_start, starts, q_ref, *refs):
    piece_refs = refs[: len(starts)]
    (
        tile_ref, peak_ref, summed_ref, wout_ref, keep_ref, send_ref, mixed_ref,
    ) = refs[len(starts) :]
    heads = q_ref.shape[0]
    kv_width = q_ref.shape[2]
    group = heads * HEAD_DIM // kv_width
    rows = slice(q_start, q_start + CHUNK)
    upper = len(starts) * CHUNK

    def put(head, summed):
        ratio = summed[:, :kv_width] / summed[:, kv_width:]
        at = head // group * HEAD_DIM
        into = head * HEAD_DIM
        mixed_ref[:, into : into + HEAD_DIM] = ratio[:, at : at + HEAD_DIM].astype(bf16)

    @pl.when(lax.axis_index("sp") == 0)
    def _():
        for head in range(heads):
            put(head, summed_ref[head])

    @pl.when(lax.axis_index("sp") > 0)
    def _():
        pieces = [
            ref[start : start + CHUNK, :] for ref, start in zip(piece_refs, starts, strict=True)
        ]
        keys = jnp.concatenate([piece[:, :kv_width] for piece in pieces], axis=0)
        values = jnp.concatenate([piece[:, kv_width:] for piece in pieces], axis=0)
        values = jnp.concatenate([values, jnp.ones_like(values)], axis=1)
        scores = lax.dot_general(
            q_ref[:, rows, :].reshape(heads * CHUNK, kv_width), keys, (((1,), (1,)), ((), ())),
            preferred_element_type=f32,
        ).reshape(heads, CHUNK, upper)
        scores = scores + tile_ref[:, :, :upper]
        before = peak_ref[...]
        peaks = jnp.max(scores, axis=-1, keepdims=True)
        peaks = jnp.maximum(before, jnp.broadcast_to(peaks, before.shape))
        spread = jnp.concatenate([peaks] * len(starts), axis=2)
        expons = jnp.exp2(scores - spread).astype(bf16)
        summed = jnp.dot(
            expons.reshape(heads * CHUNK, upper), values, preferred_element_type=f32
        ).reshape(summed_ref.shape)
        scale = jnp.exp2(before - peaks)
        for head in range(heads):
            wide = jnp.concatenate([scale[head]] * (summed.shape[2] // LANES), axis=1)
            put(head, summed_ref[head] * wide + summed[head])

    out_projection(block, layer_index, mixed_ref, wout_ref, keep_ref, send_ref)


def add_kernel(a_ref, b_ref, out_ref):
    out_ref[...] = (a_ref[...].astype(f32) + b_ref[...].astype(f32)).astype(bf16)


def split_add_kernel(block, bit, a_ref, b_ref, keep_ref, send_ref):
    parity = (lax.axis_index("tp") >> bit) & 1
    for index in range(keep_ref.shape[1] // block):
        into = slice(index * block, (index + 1) * block)
        for target, side in ((send_ref, 1 - parity), (keep_ref, parity)):
            cols = pl.ds(pl.multiple_of((2 * index + side) * block, LANES), block)
            target[:, into] = (
                a_ref[:, cols].astype(f32) + b_ref[:, cols].astype(f32)
            ).astype(bf16)


def residual_kernel(block, start, x_ref, *refs):
    out_ref = refs[-1]
    parity = lax.axis_index("tp") % 2
    at = 0
    for a_ref, b_ref in zip(refs[:-1:2], refs[1:-1:2], strict=True):
        count = a_ref.shape[0]
        for index in range(out_ref.shape[1] // block):
            into = slice(index * block, (index + 1) * block)
            cols = pl.ds(pl.multiple_of((2 * index + parity) * block, LANES), block)
            added = a_ref[:, into].astype(f32) + b_ref[:, into].astype(f32)
            held = x_ref[start + at : start + at + count, cols].astype(f32)
            out_ref[at : at + count, into] = (held + added).astype(bf16)
        at += count


def result_kernel(block, places, *refs):
    out_hbm, held_ref, sems = refs[-3:]
    cols = pl.ds(pl.multiple_of((lax.axis_index("tp") // 2) * block, LANES), block)
    copies = []
    for index, (start, inner) in enumerate(places):
        x_ref, a_ref, b_ref = refs[3 * index : 3 * index + 3]
        count = a_ref.shape[0]
        added = a_ref[...].astype(f32) + b_ref[...].astype(f32)
        held = x_ref[inner : inner + count, cols].astype(f32)
        held_ref[start : start + count, :] = (held + added).astype(bf16)
        span = pl.ds(start, count)
        copy = pltpu.make_async_copy(held_ref.at[span, :], out_hbm.at[span, :], sems.at[index])
        copy.start()
        copies.append(copy)
    for copy in copies:
        copy.wait()


def swapped(value, bit):
    size = lax.axis_size("tp")
    return lax.ppermute(value, "tp", [(d, d ^ (1 << bit)) for d in range(size)])


def passed_along(value, closed):
    size = lax.axis_size("sp")
    edges = [(d, (d + 1) % size) for d in range(size if closed else size - 1)]
    return lax.ppermute(value, "sp", edges)


def kept_in_hbm(*arrays):
    return [pltpu.with_memory_space_constraint(array, pltpu.HBM) for array in arrays]


def layers(stream, attn_gain, w_query, w_key, w_value, w_out, query_gain, key_gain, rel_bias):
    rows, width = stream.shape
    bits = lax.axis_size("tp").bit_length() - 1
    block = width // lax.axis_size("tp")
    half = width // 2
    query_width = w_query.shape[2]
    kv_width = w_key.shape[2]
    heads = query_width // HEAD_DIM
    parts = rows // CHUNK
    order = list(reversed(range(parts)))

    def queries(layer_index, normed):
        count = normed.shape[0]
        return pl.pallas_call(
            functools.partial(query_kernel, layer_index),
            out_shape=out((heads, count, kv_width)),
            in_specs=[whole] * 3,
            out_specs=whole,
            compiler_params=params(),
            cost_estimate=cost(2e9, 2 * width * query_width),
            name="queries",
        )(normed, w_query, query_gain)

    def attention(layer_index, part, inner, count, query, q_start, pieces, starts):
        return pl.pallas_call(
            functools.partial(
                attention_kernel, block, layer_index, q_start, inner,
                STEPS[count], starts, max(0, PIECES - 1 - part),
            ),
            out_shape=[out((count, half))] * 2,
            in_specs=[whole] * (PIECES + 3),
            out_specs=[whole, whole],
            scratch_shapes=[pltpu.VMEM((count, query_width), bf16)],
            compiler_params=params(),
            cost_estimate=cost(
                2 * CHUNK * query_width * (width + 4 * WINDOW), 2 * width * query_width
            ),
            name="attention",
        )(query, *pieces, tiles[layer_index], w_out)

    def own_part(layer_index, part, query, q_start, pieces, starts):
        prior = max(0, PIECES - 1 - part)
        return pl.pallas_call(
            functools.partial(own_kernel, q_start, starts[prior:]),
            out_shape=[
                out((heads, CHUNK, LANES), f32), out((heads, CHUNK, 2 * kv_width), f32)
            ],
            in_specs=[whole] * (PIECES - prior + 2),
            out_specs=[whole, whole],
            compiler_params=params(),
            cost_estimate=cost(5e8, 1e6),
            name="own_part",
        )(query, *pieces[prior:], tiles[layer_index])

    def joined(layer_index, part, query, q_start, pieces, starts, own):
        prior = max(0, PIECES - 1 - part)
        return pl.pallas_call(
            functools.partial(joined_kernel, block, layer_index, q_start, starts[:prior]),
            out_shape=[out((CHUNK, half))] * 2,
            in_specs=[whole] * (prior + 5),
            out_specs=[whole, whole],
            scratch_shapes=[pltpu.VMEM((CHUNK, query_width), bf16)],
            compiler_params=params(),
            cost_estimate=cost(1e9, 2 * width * query_width),
            name="joined",
        )(query, *pieces[:prior], tiles[layer_index], *own, w_out)

    normed, kv, table = pl.pallas_call(
        first_norm_kernel,
        out_shape=[
            out((rows, width)), out((rows, 2 * kv_width)), out(rel_bias.shape, f32)
        ],
        in_specs=[in_hbm] * 6,
        out_specs=[whole] * 3,
        scratch_shapes=[
            pltpu.VMEM(stream.shape, bf16),
            pltpu.VMEM(attn_gain.shape, f32),
            pltpu.VMEM((width, kv_width), bf16),
            pltpu.VMEM((width, kv_width), bf16),
            pltpu.VMEM(key_gain.shape, f32),
            pltpu.SemaphoreType.DMA((4,)),
            pltpu.SemaphoreType.DMA((5,)),
        ],
        compiler_params=params(),
        cost_estimate=cost(3e9, 4 * rows * width),
        name="norm_kv_first",
    )(*kept_in_hbm(stream, attn_gain, w_key, w_value, key_gain, rel_bias))
    kv_prior = passed_along(kv[rows - REACH :], False)
    query = queries(0, normed)
    tiles = []
    for layer_index in range(LAYERS):
        tiles.append(
            pl.pallas_call(
                functools.partial(bias_kernel, layer_index),
                out_shape=out((heads, CHUNK, WINDOW), f32),
                in_specs=[whole],
                out_specs=whole,
                compiler_params=params(),
                cost_estimate=cost(2e9, 1e6),
                name="bias_tiles",
            )(table)
        )

    mine, other, kvs, normeds = {}, {}, {}, {}
    for part in order:
        pieces, starts = [], []
        for index in range(PIECES):
            behind = part - (PIECES - 1) + index
            pieces.append(kv_prior if behind < 0 else kv)
            starts.append((behind + PIECES - 1 if behind < 0 else behind) * CHUNK)
        sums = []
        for inner, count in split_rows(False):
            if part < PIECES - 1:
                own = own_part(0, part, query, part * CHUNK, pieces, starts)
                keep, send = joined(0, part, query, part * CHUNK, pieces, starts, own)
            else:
                keep, send = attention(
                    0, part, inner, count, query, part * CHUNK + inner, pieces, starts
                )
            received = swapped(send, 0)
            for bit in range(1, bits):
                summed = pl.pallas_call(
                    add_kernel,
                    out_shape=out((count, half)),
                    in_specs=[whole, whole],
                    out_specs=whole,
                    compiler_params=params(),
                    name="add",
                )(keep, received)
                keep, received = summed, swapped(summed, bit)
            sums += [keep, received]
        mine[part] = pl.pallas_call(
            functools.partial(residual_kernel, block, part * CHUNK),
            out_shape=out((CHUNK, half)),
            in_specs=[whole] * (1 + len(sums)),
            out_specs=whole,
            compiler_params=params(),
            name="residual",
        )(stream, *sums)
        other[part] = swapped(mine[part], 0)

    priors = {}
    for part in order:
        normeds[part], kvs[part] = pl.pallas_call(
            functools.partial(next_norm_kernel, 1, block),
            out_shape=[out((CHUNK, width)), out((CHUNK, 2 * kv_width))],
            in_specs=[whole] * 6,
            out_specs=[whole, whole],
            compiler_params=params(),
            cost_estimate=cost(4 * CHUNK * width * kv_width, 4 * CHUNK * width),
            name="norm_kv_next",
        )(mine[part], other[part], attn_gain, w_key, w_value, key_gain)
        if part >= parts - (PIECES - 1):
            priors[part - parts] = passed_along(kvs[part], True)

    places, outs = [], []
    for part in order:
        query = queries(1, normeds[part])
        pieces = []
        for index in range(PIECES):
            behind = part - (PIECES - 1) + index
            pieces.append(priors[behind] if behind < 0 else kvs[behind])
        for inner, count in split_rows(False):
            if part == 0:
                own = own_part(1, part, query, 0, pieces, [0] * PIECES)
                keep, send = joined(1, part, query, 0, pieces, [0] * PIECES, own)
            else:
                keep, send = attention(1, part, inner, count, query, inner, pieces, [0] * PIECES)
            received = swapped(send, 0)
            for bit in range(1, bits):
                left = keep.shape[1] // 2
                keep, send = pl.pallas_call(
                    functools.partial(split_add_kernel, block, bit),
                    out_shape=[out((count, left))] * 2,
                    in_specs=[whole, whole],
                    out_specs=[whole, whole],
                    compiler_params=params(),
                    name="split_add",
                )(keep, received)
                received = swapped(send, bit)
            places.append((part * CHUNK + inner, inner))
            outs += [mine[part], keep, received]

    return pl.pallas_call(
        functools.partial(result_kernel, block, places),
        out_shape=out((rows, block)),
        in_specs=[whole] * len(outs),
        out_specs=in_hbm,
        scratch_shapes=[pltpu.VMEM((rows, block), bf16), pltpu.SemaphoreType.DMA((len(places),))],
        compiler_params=params(),
        name="result",
    )(*outs)


def split_rows(fine):
    return [(at, SEG) for at in range(0, CHUNK, SEG)] if fine else [(0, CHUNK)]


STEPS = {CHUNK: 1, SEG: 2}


def solution(mesh):
    return jax.shard_map(
        layers,
        mesh=mesh,
        in_specs=(
            P("sp", None),
            P(),
            P(None, None, "tp"),
            P(None, None, "tp"),
            P(None, None, "tp"),
            P(None, "tp", None),
            P(),
            P(),
            P(None, "tp", None),
        ),
        out_specs=P("sp", "tp"),
        check_vma=False,
    )
```

```python
import functools

import jax
import jax.numpy as jnp
from jax import lax
from jax.experimental import pallas as pl
from jax.experimental.pallas import tpu as pltpu
from jax.sharding import PartitionSpec as P


HEAD_DIM = 64
SEG = 64
LEFT = 4
CLIP = 128
LAYERS = 2

REACH = LEFT * SEG
CHUNK = 2 * SEG
PIECES = REACH // CHUNK + 1
WINDOW = REACH + CHUNK
LINE = WINDOW + CHUNK
LANES = 128

norm_eps = 1e-06
masked_score = -1e30

LOG2_E = 1.4426950408889634

bf16 = jnp.bfloat16
f32 = jnp.float32

whole = pl.BlockSpec(memory_space=pltpu.VMEM)
in_hbm = pl.BlockSpec(memory_space=pltpu.HBM)


def params():
    return pltpu.CompilerParams(vmem_limit_bytes=12 * 1024 * 1024)


def cost(flops, moved):
    return pl.CostEstimate(flops=int(flops), bytes_accessed=int(moved), transcendentals=0)


def out(shape, dtype=bf16):
    return jax.ShapeDtypeStruct(shape, dtype)


def head_norm(flat, gain_row):
    width = flat.shape[1]
    step = min(width, LANES)
    row = lax.broadcasted_iota(jnp.int32, (step, step), 0) // HEAD_DIM
    col = lax.broadcasted_iota(jnp.int32, (step, step), 1) // HEAD_DIM
    mean_of = jnp.where(row == col, 1.0 / HEAD_DIM, 0.0).astype(bf16)
    gain = jnp.concatenate([gain_row] * (step // HEAD_DIM), axis=1)
    pieces = []
    for lower in range(0, width, step):
        part = flat[:, lower : lower + step]
        squared = part * part
        high = squared.astype(bf16)
        low = (squared - high.astype(f32)).astype(bf16)
        mean = jnp.dot(high, mean_of, preferred_element_type=f32) + jnp.dot(
            low, mean_of, preferred_element_type=f32
        )
        pieces.append(part * lax.rsqrt(mean + norm_eps) * gain)
    return pieces


def key_value_body(normed, weights, key_gain_row, kv_refs):
    flat = jnp.dot(normed, weights, preferred_element_type=f32)
    kv_width = flat.shape[1] // 2
    keys = head_norm(flat[:, :kv_width], key_gain_row)[0]
    values = flat[:, kv_width:]
    both = jnp.concatenate([keys, values], axis=1).astype(bf16)
    for index, kv_ref in enumerate(kv_refs):
        kv_ref[...] = both[index * CHUNK : (index + 1) * CHUNK, :]


def first_norm_kernel(
    x_hbm, gain_hbm, wk_hbm, wv_hbm, kg_hbm, table_hbm, normed_ref, table_ref, *refs,
):
    *kv_refs, x_ref, gain_ref, weight_ref, kg_ref, row_sems, sems = refs
    steps = row_sems.shape[0]
    share = x_ref.shape[0] // steps
    row_copies = []
    for index in range(steps):
        at = pl.ds(index * share, share)
        row_copies.append(
            pltpu.make_async_copy(x_hbm.at[at, :], x_ref.at[at, :], row_sems.at[index])
        )
    gain_copy = pltpu.make_async_copy(gain_hbm, gain_ref, sems.at[0])
    late = [
        pltpu.make_async_copy(wk_hbm.at[0], weight_ref.at[0], sems.at[1]),
        pltpu.make_async_copy(wv_hbm.at[0], weight_ref.at[1], sems.at[2]),
        pltpu.make_async_copy(kg_hbm, kg_ref, sems.at[3]),
        pltpu.make_async_copy(table_hbm, table_ref, sems.at[4]),
    ]
    for copy in [gain_copy] + row_copies + late:
        copy.start()
    gain_copy.wait()
    gain = gain_ref[0:1, :]
    for index, copy in enumerate(row_copies):
        copy.wait()
        at = slice(index * share, (index + 1) * share)
        current = x_ref[at, :].astype(f32)
        mean = jnp.mean(current * current, axis=-1, keepdims=True)
        normed_ref[at, :] = (current * lax.rsqrt(mean + norm_eps) * gain).astype(bf16)
    for copy in late:
        copy.wait()
    weights = jnp.concatenate([weight_ref[0], weight_ref[1]], axis=1)
    key_value_body(normed_ref[...], weights, kg_ref[0:1, :], kv_refs)


def next_norm_kernel(
    layer_index, block, mine_ref, other_ref, gain_ref, wk_ref, wv_ref, kg_ref,
    normed_ref, kv_ref,
):
    parity = lax.axis_index("tp") % 2
    mine = mine_ref[...].astype(f32)
    other = other_ref[...].astype(f32)
    total = jnp.sum(mine * mine, axis=-1, keepdims=True)
    total = total + jnp.sum(other * other, axis=-1, keepdims=True)
    scale = lax.rsqrt(total / (2 * mine.shape[1]) + norm_eps)
    for index in range(mine.shape[1] // block):
        for held, side in ((mine, parity), (other, 1 - parity)):
            cols = pl.ds(pl.multiple_of((2 * index + side) * block, LANES), block)
            piece = held[:, index * block : (index + 1) * block]
            gain = gain_ref[layer_index : layer_index + 1, cols]
            normed_ref[:, cols] = (piece * scale * gain).astype(bf16)
    key_value_body(
        normed_ref[...],
        jnp.concatenate([wk_ref[layer_index], wv_ref[layer_index]], axis=1),
        kg_ref[layer_index : layer_index + 1, :], [kv_ref],
    )


def query_kernel(layer_index, normed_ref, wq_ref, qg_ref, q_ref):
    flat = jnp.dot(normed_ref[...], wq_ref[layer_index], preferred_element_type=f32)
    query_body(flat, qg_ref[layer_index : layer_index + 1, :], q_ref)


def query_body(flat, gain_row, q_ref):
    pieces = head_norm(flat, gain_row * (HEAD_DIM**-0.5 * LOG2_E))
    kv_width = q_ref.shape[2]
    group = q_ref.shape[0] * HEAD_DIM // kv_width
    lanes = pieces[0].shape[1]
    for head in range(q_ref.shape[0]):
        at = head * HEAD_DIM
        piece = pieces[at // lanes][:, at % lanes : at % lanes + HEAD_DIM]
        before = head // group * HEAD_DIM
        after = kv_width - HEAD_DIM - before
        rows = piece.shape[0]
        spread = [jnp.zeros((rows, before), f32)] if before else []
        spread += [piece] + ([jnp.zeros((rows, after), f32)] if after else [])
        q_ref[head] = jnp.concatenate(spread, axis=1).astype(bf16)


def bias_kernel(layer_index, table_ref, tile_ref):
    heads, entries = table_ref.shape[1:]
    source = lax.broadcasted_iota(jnp.int32, (entries, LINE), 0)
    offset = lax.broadcasted_iota(jnp.int32, (entries, LINE), 1)
    distance = jnp.clip(WINDOW - 1 - offset, -CLIP, CLIP) + CLIP
    onehot = (source == distance).astype(f32)
    query_seg = lax.broadcasted_iota(jnp.int32, (CHUNK, WINDOW), 0) // SEG
    key_seg = lax.broadcasted_iota(jnp.int32, (CHUNK, WINDOW), 1) // SEG
    inside = (key_seg >= query_seg) & (key_seg <= query_seg + LEFT)
    line = jnp.dot(
        table_ref[layer_index] * LOG2_E, onehot, precision=lax.Precision.HIGHEST,
        preferred_element_type=f32,
    )
    for head in range(heads):
        spread = jnp.broadcast_to(line[head : head + 1, :], (CHUNK, LINE))
        rolled = pltpu.roll(spread, LINE - CHUNK + 1, 1, stride=1, stride_axis=0)
        tile_ref[head] = jnp.where(inside, rolled[:, :WINDOW], masked_score)


def attention_kernel(
    block, layer_index, q_start, row_start, step, starts, prior, q_ref, *refs,
):
    piece_refs = refs[:PIECES]
    tile_ref, wout_ref, *out_refs, mixed_ref = refs[PIECES:]
    heads = q_ref.shape[0]
    kv_width = q_ref.shape[2]
    group = heads * HEAD_DIM // kv_width
    count = mixed_ref.shape[0]
    rows = slice(q_start, q_start + count)

    pieces = [
        ref[start : start + CHUNK, :] for ref, start in zip(piece_refs, starts, strict=True)
    ]
    keys = jnp.concatenate([piece[:, :kv_width] for piece in pieces], axis=0)
    values = jnp.concatenate([piece[:, kv_width:] for piece in pieces], axis=0)
    values = jnp.concatenate([values, jnp.ones_like(values)], axis=1)
    key_index = lax.broadcasted_iota(jnp.int32, (1, WINDOW), 1)
    outside = (key_index < prior * CHUNK) & (lax.axis_index("sp") == 0)
    outside = jnp.where(outside, masked_score, 0.0)
    for first in range(0, heads, step):
        stacked = jnp.concatenate([q_ref[first + index, rows, :] for index in range(step)], axis=0)
        scores = lax.dot_general(
            stacked, keys, (((1,), (1,)), ((), ())), preferred_element_type=f32
        )
        expons = []
        for index in range(step):
            score = scores[index * count : (index + 1) * count, :]
            score = score + tile_ref[first + index, row_start : row_start + count, :]
            if prior:
                score = score + outside
            peak = jnp.max(score, axis=-1, keepdims=True)
            expons.append(jnp.exp2(score - peak).astype(bf16))
        summed = jnp.dot(
            jnp.concatenate(expons, axis=0), values, preferred_element_type=f32
        )
        ratio = summed[:, :kv_width] / summed[:, kv_width:]
        for index in range(step):
            at = (first + index) // group * HEAD_DIM
            into = (first + index) * HEAD_DIM
            part = ratio[index * count : (index + 1) * count, at : at + HEAD_DIM]
            mixed_ref[:, into : into + HEAD_DIM] = part.astype(bf16)

    out_projection(block, layer_index, mixed_ref, wout_ref, *out_refs)


def out_projection(block, layer_index, mixed_ref, wout_ref, keep_ref, send_ref=None):
    parity = lax.axis_index("tp") % 2
    mixed = mixed_ref[...]

    def project(place):
        cols = pl.ds(pl.multiple_of(place * block, LANES), block)
        value = jnp.dot(mixed, wout_ref[layer_index, :, cols], preferred_element_type=f32)
        return value.astype(bf16)

    if send_ref is None and keep_ref.shape[1] == block:
        chip = lax.axis_index("tp") // 2
        keep_ref[...] = project(2 * (1 - chip) + 1 - parity)
        return
    for index in range(keep_ref.shape[1] // block):
        into = slice(index * block, (index + 1) * block)
        if send_ref is None:
            keep_ref[:, into] = project(2 * index + 1 - parity)
        else:
            send_ref[:, into] = project(2 * index + 1 - parity)
            keep_ref[:, into] = project(2 * index + parity)


def keep_kernel(block, layer_index, mixed_ref, wout_ref, keep_ref):
    parity = lax.axis_index("tp") % 2
    mixed = mixed_ref[...]
    for index in range(keep_ref.shape[1] // block):
        cols = pl.ds(pl.multiple_of((2 * index + parity) * block, LANES), block)
        value = jnp.dot(mixed, wout_ref[layer_index, :, cols], preferred_element_type=f32)
        keep_ref[:, index * block : (index + 1) * block] = value.astype(bf16)


def project_kernel(block, layer_index, which, mixed_ref, wout_ref, *out_refs):
    parity = lax.axis_index("tp") % 2
    chip = lax.axis_index("tp") // 2
    mixed = mixed_ref[...]
    for (near_chip, near_core), target in zip(which, out_refs, strict=True):
        place = 2 * (chip if near_chip else 1 - chip) + (parity if near_core else 1 - parity)
        cols = pl.ds(pl.multiple_of(place * block, LANES), block)
        value = jnp.dot(mixed, wout_ref[layer_index, :, cols], preferred_element_type=f32)
        target[...] = value.astype(bf16)


def own_kernel(q_start, starts, q_ref, *refs):
    piece_refs = refs[: len(starts)]
    tile_ref, peak_ref, summed_ref = refs[len(starts) :]
    kv_width = q_ref.shape[2]
    rows = slice(q_start, q_start + CHUNK)
    pieces = [
        ref[start : start + CHUNK, :] for ref, start in zip(piece_refs, starts, strict=True)
    ]
    keys = jnp.concatenate([piece[:, :kv_width] for piece in pieces], axis=0)
    values = jnp.concatenate([piece[:, kv_width:] for piece in pieces], axis=0)
    values = jnp.concatenate([values, jnp.ones_like(values)], axis=1)
    lower = WINDOW - len(starts) * CHUNK
    heads = q_ref.shape[0]
    scores = lax.dot_general(
        q_ref[:, rows, :].reshape(heads * CHUNK, kv_width), keys, (((1,), (1,)), ((), ())),
        preferred_element_type=f32,
    ).reshape(heads, CHUNK, keys.shape[0])
    scores = scores + tile_ref[:, :, lower:]
    peaks = jnp.max(scores, axis=-1, keepdims=True)
    expons = jnp.exp2(scores - peaks).astype(bf16)
    peak_ref[...] = jnp.broadcast_to(peaks, peak_ref.shape)
    summed = jnp.dot(
        expons.reshape(heads * CHUNK, keys.shape[0]), values, preferred_element_type=f32
    )
    summed_ref[...] = summed.reshape(summed_ref.shape)


def joined_kernel(block, layer_index, q_start, starts, q_ref, *refs):
    piece_refs = refs[: len(starts)]
    tile_ref, peak_ref, summed_ref, wout_ref, *out_refs, mixed_ref = refs[len(starts) :]
    heads = q_ref.shape[0]
    kv_width = q_ref.shape[2]
    group = heads * HEAD_DIM // kv_width
    rows = slice(q_start, q_start + CHUNK)
    upper = len(starts) * CHUNK

    def put(head, summed):
        ratio = summed[:, :kv_width] / summed[:, kv_width:]
        at = head // group * HEAD_DIM
        into = head * HEAD_DIM
        mixed_ref[:, into : into + HEAD_DIM] = ratio[:, at : at + HEAD_DIM].astype(bf16)

    @pl.when(lax.axis_index("sp") == 0)
    def _():
        for head in range(heads):
            put(head, summed_ref[head])

    @pl.when(lax.axis_index("sp") > 0)
    def _():
        pieces = [
            ref[start : start + CHUNK, :] for ref, start in zip(piece_refs, starts, strict=True)
        ]
        keys = jnp.concatenate([piece[:, :kv_width] for piece in pieces], axis=0)
        values = jnp.concatenate([piece[:, kv_width:] for piece in pieces], axis=0)
        values = jnp.concatenate([values, jnp.ones_like(values)], axis=1)
        scores = lax.dot_general(
            q_ref[:, rows, :].reshape(heads * CHUNK, kv_width), keys, (((1,), (1,)), ((), ())),
            preferred_element_type=f32,
        ).reshape(heads, CHUNK, upper)
        scores = scores + tile_ref[:, :, :upper]
        before = peak_ref[...]
        peaks = jnp.max(scores, axis=-1, keepdims=True)
        peaks = jnp.maximum(before, jnp.broadcast_to(peaks, before.shape))
        spread = jnp.concatenate([peaks] * len(starts), axis=2)
        expons = jnp.exp2(scores - spread).astype(bf16)
        summed = jnp.dot(
            expons.reshape(heads * CHUNK, upper), values, preferred_element_type=f32
        ).reshape(summed_ref.shape)
        scale = jnp.exp2(before - peaks)
        for head in range(heads):
            wide = jnp.concatenate([scale[head]] * (summed.shape[2] // LANES), axis=1)
            put(head, summed_ref[head] * wide + summed[head])

    out_projection(block, layer_index, mixed_ref, wout_ref, *out_refs)


def add_kernel(a_ref, b_ref, out_ref):
    out_ref[...] = (a_ref[...].astype(f32) + b_ref[...].astype(f32)).astype(bf16)


def split_add_kernel(block, bit, a_ref, b_ref, keep_ref, send_ref):
    parity = (lax.axis_index("tp") >> bit) & 1
    for index in range(keep_ref.shape[1] // block):
        into = slice(index * block, (index + 1) * block)
        for target, side in ((send_ref, 1 - parity), (keep_ref, parity)):
            cols = pl.ds(pl.multiple_of((2 * index + side) * block, LANES), block)
            target[:, into] = (
                a_ref[:, cols].astype(f32) + b_ref[:, cols].astype(f32)
            ).astype(bf16)


def residual_kernel(block, start, x_ref, *refs):
    out_ref = refs[-1]
    parity = lax.axis_index("tp") % 2
    at = 0
    for a_ref, b_ref in zip(refs[:-1:2], refs[1:-1:2], strict=True):
        count = a_ref.shape[0]
        for index in range(out_ref.shape[1] // block):
            into = slice(index * block, (index + 1) * block)
            cols = pl.ds(pl.multiple_of((2 * index + parity) * block, LANES), block)
            added = a_ref[:, into].astype(f32) + b_ref[:, into].astype(f32)
            held = x_ref[start + at : start + at + count, cols].astype(f32)
            out_ref[at : at + count, into] = (held + added).astype(bf16)
        at += count


def result_kernel(block, places, *refs):
    out_hbm, held_ref, sems = refs[-3:]
    cols = pl.ds(pl.multiple_of((lax.axis_index("tp") // 2) * block, LANES), block)
    copies = []
    at = 0
    for index, (start, count, addends) in enumerate(places):
        added = sum(ref[...].astype(f32) for ref in refs[at + 1 : at + 1 + addends])
        held = refs[at][:, cols].astype(f32)
        held_ref[start : start + count, :] = (held + added).astype(bf16)
        span = pl.ds(start, count)
        copy = pltpu.make_async_copy(held_ref.at[span, :], out_hbm.at[span, :], sems.at[index])
        copy.start()
        copies.append(copy)
        at += 1 + addends
    for copy in copies:
        copy.wait()


def swapped(value, bit):
    size = lax.axis_size("tp")
    return lax.ppermute(value, "tp", [(d, d ^ (1 << bit)) for d in range(size)])


def passed_along(value, closed):
    size = lax.axis_size("sp")
    edges = [(d, (d + 1) % size) for d in range(size if closed else size - 1)]
    return lax.ppermute(value, "sp", edges)


def kept_in_hbm(*arrays):
    return [pltpu.with_memory_space_constraint(array, pltpu.HBM) for array in arrays]


def layers(stream, attn_gain, w_query, w_key, w_value, w_out, query_gain, key_gain, rel_bias):
    rows, width = stream.shape
    bits = lax.axis_size("tp").bit_length() - 1
    block = width // lax.axis_size("tp")
    half = width // 2
    query_width = w_query.shape[2]
    kv_width = w_key.shape[2]
    heads = query_width // HEAD_DIM
    parts = rows // CHUNK
    order = list(reversed(range(parts)))

    def queries(layer_index, normed):
        count = normed.shape[0]
        return pl.pallas_call(
            functools.partial(query_kernel, layer_index),
            out_shape=out((heads, count, kv_width)),
            in_specs=[whole] * 3,
            out_specs=whole,
            compiler_params=params(),
            cost_estimate=cost(2e9, 2 * width * query_width),
            name="queries",
        )(normed, w_query, query_gain)

    def attention_out(early, count):
        if early:
            return dict(
                out_shape=[out((count, early)), out((count, query_width))],
                out_specs=[whole, whole],
            )
        return dict(
            out_shape=[out((count, half))] * 2,
            out_specs=[whole, whole],
            scratch_shapes=[pltpu.VMEM((count, query_width), bf16)],
        )

    def attention(layer_index, part, inner, count, query, q_start, pieces, starts, early=0):
        return pl.pallas_call(
            functools.partial(
                attention_kernel, block, layer_index, q_start, inner,
                STEPS[count], starts, max(0, PIECES - 1 - part),
            ),
            **attention_out(early, count),
            in_specs=[whole] * (PIECES + 3),
            compiler_params=params(),
            cost_estimate=cost(
                2 * CHUNK * query_width * (width + 4 * WINDOW), 2 * width * query_width
            ),
            name="attention",
        )(query, *pieces, tiles[layer_index], w_out)

    def own_part(layer_index, part, query, q_start, pieces, starts):
        prior = max(0, PIECES - 1 - part)
        return pl.pallas_call(
            functools.partial(own_kernel, q_start, starts[prior:]),
            out_shape=[
                out((heads, CHUNK, LANES), f32), out((heads, CHUNK, 2 * kv_width), f32)
            ],
            in_specs=[whole] * (PIECES - prior + 2),
            out_specs=[whole, whole],
            compiler_params=params(),
            cost_estimate=cost(5e8, 1e6),
            name="own_part",
        )(query, *pieces[prior:], tiles[layer_index])

    def joined(layer_index, part, query, q_start, pieces, starts, own, early=0):
        prior = max(0, PIECES - 1 - part)
        return pl.pallas_call(
            functools.partial(joined_kernel, block, layer_index, q_start, starts[:prior]),
            **attention_out(early, CHUNK),
            in_specs=[whole] * (prior + 5),
            compiler_params=params(),
            cost_estimate=cost(1e9, 2 * width * query_width),
            name="joined",
        )(query, *pieces[:prior], tiles[layer_index], *own, w_out)

    def project(layer_index, mixed, which):
        return pl.pallas_call(
            functools.partial(project_kernel, block, layer_index, which),
            out_shape=[out((mixed.shape[0], block))] * len(which),
            in_specs=[whole, whole],
            out_specs=[whole] * len(which),
            compiler_params=params(),
            cost_estimate=cost(3e8, 1e6),
            name="project",
        )(mixed, w_out)

    def added(one, two):
        return pl.pallas_call(
            add_kernel,
            out_shape=out(one.shape),
            in_specs=[whole, whole],
            out_specs=whole,
            compiler_params=params(),
            name="add",
        )(one, two)

    normed, table, *kvs_first = pl.pallas_call(
        first_norm_kernel,
        out_shape=[
            out((rows, width)), out(rel_bias.shape, f32),
            *[out((CHUNK, 2 * kv_width))] * parts,
        ],
        in_specs=[in_hbm] * 6,
        out_specs=[whole] * (2 + parts),
        scratch_shapes=[
            pltpu.VMEM(stream.shape, bf16),
            pltpu.VMEM(attn_gain.shape, f32),
            pltpu.VMEM((2, width, kv_width), bf16),
            pltpu.VMEM(key_gain.shape, f32),
            pltpu.SemaphoreType.DMA((4,)),
            pltpu.SemaphoreType.DMA((5,)),
        ],
        compiler_params=params(),
        cost_estimate=cost(3e9, 4 * rows * width),
        name="norm_kv_first",
    )(*kept_in_hbm(stream, attn_gain, w_key, w_value, key_gain, rel_bias))
    first_priors = {}
    for part in order[: PIECES - 1]:
        first_priors[part - parts] = passed_along(kvs_first[part], True)
    query = queries(0, normed)
    tiles = []
    for layer_index in range(LAYERS):
        tiles.append(
            pl.pallas_call(
                functools.partial(bias_kernel, layer_index),
                out_shape=out((heads, CHUNK, WINDOW), f32),
                in_specs=[whole],
                out_specs=whole,
                compiler_params=params(),
                cost_estimate=cost(2e9, 1e6),
                name="bias_tiles",
            )(table)
        )

    mine, other, kvs, normeds = {}, {}, {}, {}
    for part in order:
        pieces, starts = [], [0] * PIECES
        for index in range(PIECES):
            behind = part - (PIECES - 1) + index
            pieces.append(first_priors[behind] if behind < 0 else kvs_first[behind])
        sums = []
        for inner, count in split_rows(False):
            if part < PIECES - 1:
                own = own_part(0, part, query, part * CHUNK, pieces, starts)
                send, mixed = joined(
                    0, part, query, part * CHUNK, pieces, starts, own, half
                )
                keep = pl.pallas_call(
                    functools.partial(keep_kernel, block, 0),
                    out_shape=out((CHUNK, half)),
                    in_specs=[whole, whole],
                    out_specs=whole,
                    compiler_params=params(),
                    cost_estimate=cost(3e8, 1e6),
                    name="keep",
                )(mixed, w_out)
            else:
                keep, send = attention(
                    0, part, inner, count, query, part * CHUNK + inner, pieces, starts
                )
            received = swapped(send, 0)
            for bit in range(1, bits):
                summed = added(keep, received)
                keep, received = summed, swapped(summed, bit)
            sums += [keep, received]
        mine[part] = pl.pallas_call(
            functools.partial(residual_kernel, block, part * CHUNK),
            out_shape=out((CHUNK, half)),
            in_specs=[whole] * (1 + len(sums)),
            out_specs=whole,
            compiler_params=params(),
            name="residual",
        )(stream, *sums)
        other[part] = swapped(mine[part], 0)

    priors = {}
    for part in order:
        normeds[part], kvs[part] = pl.pallas_call(
            functools.partial(next_norm_kernel, 1, block),
            out_shape=[out((CHUNK, width)), out((CHUNK, 2 * kv_width))],
            in_specs=[whole] * 6,
            out_specs=[whole, whole],
            compiler_params=params(),
            cost_estimate=cost(4 * CHUNK * width * kv_width, 4 * CHUNK * width),
            name="norm_kv_next",
        )(mine[part], other[part], attn_gain, w_key, w_value, key_gain)
        if part >= parts - (PIECES - 1):
            priors[part - parts] = passed_along(kvs[part], True)

    places, outs = [], []
    for part in order:
        query = queries(1, normeds[part])
        pieces = []
        for index in range(PIECES):
            behind = part - (PIECES - 1) + index
            pieces.append(priors[behind] if behind < 0 else kvs[behind])
        early = block if bits == 2 and part == 0 else 0
        if part == 0:
            own = own_part(1, part, query, 0, pieces, [0] * PIECES)
            keep, send = joined(1, part, query, 0, pieces, [0] * PIECES, own, early)
        else:
            keep, send = attention(
                1, part, 0, CHUNK, query, 0, pieces, [0] * PIECES, early
            )
        if early:
            first, mixed = keep, send
            received = swapped(first, 0)
            send = project(1, mixed, ((False, True),))[0]
            summed = added(send, received)
            received = swapped(summed, 1)
            keep, other = project(1, mixed, ((True, True), (True, False)))
            aside = swapped(other, 0)
            addends = [keep, aside, received]
        else:
            received = swapped(send, 0)
            for bit in range(1, bits):
                left = keep.shape[1] // 2
                keep, send = pl.pallas_call(
                    functools.partial(split_add_kernel, block, bit),
                    out_shape=[out((CHUNK, left))] * 2,
                    in_specs=[whole, whole],
                    out_specs=[whole, whole],
                    compiler_params=params(),
                    name="split_add",
                )(keep, received)
                received = swapped(send, bit)
            addends = [keep, received]
        places.append((part * CHUNK, CHUNK, len(addends)))
        outs += [mine[part], *addends]

    return pl.pallas_call(
        functools.partial(result_kernel, block, places),
        out_shape=out((rows, block)),
        in_specs=[whole] * len(outs),
        out_specs=in_hbm,
        scratch_shapes=[pltpu.VMEM((rows, block), bf16), pltpu.SemaphoreType.DMA((len(places),))],
        compiler_params=params(),
        name="result",
    )(*outs)


def split_rows(fine):
    return [(at, SEG) for at in range(0, CHUNK, SEG)] if fine else [(0, CHUNK)]


STEPS = {CHUNK: 1, SEG: 2}


def solution(mesh):
    return jax.shard_map(
        layers,
        mesh=mesh,
        in_specs=(
            P("sp", None),
            P(),
            P(None, None, "tp"),
            P(None, None, "tp"),
            P(None, None, "tp"),
            P(None, "tp", None),
            P(),
            P(),
            P(None, "tp", None),
        ),
        out_specs=P("sp", "tp"),
        check_vma=False,
    )
```

```python
import functools

import jax
import jax.numpy as jnp
from jax import lax
from jax.experimental import pallas as pl
from jax.experimental.pallas import tpu as pltpu
from jax.sharding import PartitionSpec as P


HEAD_DIM = 64
SEG = 64
LEFT = 4
CLIP = 128
LAYERS = 2

REACH = LEFT * SEG
CHUNK = 2 * SEG
PIECES = REACH // CHUNK + 1
WINDOW = REACH + CHUNK
LINE = WINDOW + CHUNK
LANES = 128

norm_eps = 1e-06
masked_score = -1e30

LOG2_E = 1.4426950408889634

bf16 = jnp.bfloat16
f32 = jnp.float32

whole = pl.BlockSpec(memory_space=pltpu.VMEM)
in_hbm = pl.BlockSpec(memory_space=pltpu.HBM)


def params():
    return pltpu.CompilerParams(vmem_limit_bytes=12 * 1024 * 1024)


def cost(flops, moved):
    return pl.CostEstimate(flops=int(flops), bytes_accessed=int(moved), transcendentals=0)


def out(shape, dtype=bf16):
    return jax.ShapeDtypeStruct(shape, dtype)


def head_norm(flat, gain_row):
    width = flat.shape[1]
    step = min(width, LANES)
    row = lax.broadcasted_iota(jnp.int32, (step, step), 0) // HEAD_DIM
    col = lax.broadcasted_iota(jnp.int32, (step, step), 1) // HEAD_DIM
    mean_of = jnp.where(row == col, 1.0 / HEAD_DIM, 0.0).astype(bf16)
    gain = jnp.concatenate([gain_row] * (step // HEAD_DIM), axis=1)
    pieces = []
    for lower in range(0, width, step):
        part = flat[:, lower : lower + step]
        squared = part * part
        high = squared.astype(bf16)
        low = (squared - high.astype(f32)).astype(bf16)
        mean = jnp.dot(high, mean_of, preferred_element_type=f32) + jnp.dot(
            low, mean_of, preferred_element_type=f32
        )
        pieces.append(part * lax.rsqrt(mean + norm_eps) * gain)
    return pieces


def key_value_body(normed, weights, key_gain_row, kv_refs):
    flat = jnp.dot(normed, weights, preferred_element_type=f32)
    kv_width = flat.shape[1] // 2
    keys = head_norm(flat[:, :kv_width], key_gain_row)[0]
    values = flat[:, kv_width:]
    both = jnp.concatenate([keys, values], axis=1).astype(bf16)
    for index, kv_ref in enumerate(kv_refs):
        kv_ref[...] = both[index * CHUNK : (index + 1) * CHUNK, :]


def first_norm_kernel(
    x_hbm, gain_hbm, wk_hbm, wv_hbm, kg_hbm, table_hbm,
    normed_ref, kv_ref, gain_ref, weight_ref, kg_ref, table_ref,
    x_ref, row_sems, sems,
):
    steps = row_sems.shape[0]
    rest = x_hbm.shape[0] - x_ref.shape[0]
    share = x_ref.shape[0] // steps
    row_copies = []
    for index in range(steps):
        at = pl.ds(index * share, share)
        source = x_hbm.at[pl.ds(rest + index * share, share), :]
        row_copies.append(
            pltpu.make_async_copy(source, x_ref.at[at, :], row_sems.at[index])
        )
    gain_copy = pltpu.make_async_copy(gain_hbm, gain_ref, sems.at[0])
    weight_copies = [
        pltpu.make_async_copy(wk_hbm.at[0], weight_ref.at[0], sems.at[1]),
        pltpu.make_async_copy(wv_hbm.at[0], weight_ref.at[1], sems.at[2]),
        pltpu.make_async_copy(kg_hbm, kg_ref, sems.at[3]),
    ]
    late = [
        pltpu.make_async_copy(table_hbm, table_ref, sems.at[4]),
    ]
    for copy in [gain_copy] + row_copies + weight_copies + late:
        copy.start()
    gain_copy.wait()
    gain = gain_ref[0:1, :]
    for index, copy in enumerate(row_copies):
        copy.wait()
        at = slice(index * share, (index + 1) * share)
        normed_ref[at, :] = normalized(x_ref[at, :], gain)
    for copy in weight_copies:
        copy.wait()
    weights = jnp.concatenate([weight_ref[0], weight_ref[1]], axis=1)
    key_value_body(normed_ref[...], weights, kg_ref[0:1, :], [kv_ref])
    for copy in late:
        copy.wait()


def normalized(rows, gain):
    current = rows.astype(f32)
    mean = jnp.mean(current * current, axis=-1, keepdims=True)
    return (current * lax.rsqrt(mean + norm_eps) * gain).astype(bf16)


def rest_norm_kernel(x_ref, gain_ref, weight_ref, kg_ref, *refs):
    parts = len(refs) // 2
    weights = jnp.concatenate([weight_ref[0], weight_ref[1]], axis=1)
    for index in range(parts):
        at = slice(index * CHUNK, (index + 1) * CHUNK)
        refs[index][...] = normalized(x_ref[at, :], gain_ref[0:1, :])
        key_value_body(refs[index][...], weights, kg_ref[0:1, :], [refs[parts + index]])


def next_norm_kernel(
    layer_index, block, mine_ref, other_ref, gain_ref, wk_ref, wv_ref, kg_ref,
    normed_ref, kv_ref,
):
    parity = lax.axis_index("tp") % 2
    mine = mine_ref[...].astype(f32)
    other = other_ref[...].astype(f32)
    total = jnp.sum(mine * mine, axis=-1, keepdims=True)
    total = total + jnp.sum(other * other, axis=-1, keepdims=True)
    scale = lax.rsqrt(total / (2 * mine.shape[1]) + norm_eps)
    for index in range(mine.shape[1] // block):
        for held, side in ((mine, parity), (other, 1 - parity)):
            cols = pl.ds(pl.multiple_of((2 * index + side) * block, LANES), block)
            piece = held[:, index * block : (index + 1) * block]
            gain = gain_ref[layer_index : layer_index + 1, cols]
            normed_ref[:, cols] = (piece * scale * gain).astype(bf16)
    key_value_body(
        normed_ref[...],
        jnp.concatenate([wk_ref[layer_index], wv_ref[layer_index]], axis=1),
        kg_ref[layer_index : layer_index + 1, :], [kv_ref],
    )


def query_kernel(layer_index, normed_ref, wq_ref, qg_ref, *refs):
    q_ref = refs[-1]
    flat = jnp.dot(normed_ref[...], wq_ref[layer_index], preferred_element_type=f32)
    query_body(flat, qg_ref[layer_index : layer_index + 1, :], q_ref)


def query_body(flat, gain_row, q_ref):
    pieces = head_norm(flat, gain_row * (HEAD_DIM**-0.5 * LOG2_E))
    kv_width = q_ref.shape[2]
    group = q_ref.shape[0] * HEAD_DIM // kv_width
    lanes = pieces[0].shape[1]
    for head in range(q_ref.shape[0]):
        at = head * HEAD_DIM
        piece = pieces[at // lanes][:, at % lanes : at % lanes + HEAD_DIM]
        before = head // group * HEAD_DIM
        after = kv_width - HEAD_DIM - before
        rows = piece.shape[0]
        spread = [jnp.zeros((rows, before), f32)] if before else []
        spread += [piece] + ([jnp.zeros((rows, after), f32)] if after else [])
        q_ref[head] = jnp.concatenate(spread, axis=1).astype(bf16)


def bias_kernel(layer_index, table_ref, *refs):
    tile_ref = refs[-1]
    heads, entries = table_ref.shape[1:]
    source = lax.broadcasted_iota(jnp.int32, (entries, LINE), 0)
    offset = lax.broadcasted_iota(jnp.int32, (entries, LINE), 1)
    distance = jnp.clip(WINDOW - 1 - offset, -CLIP, CLIP) + CLIP
    onehot = (source == distance).astype(f32)
    query_seg = lax.broadcasted_iota(jnp.int32, (CHUNK, WINDOW), 0) // SEG
    key_seg = lax.broadcasted_iota(jnp.int32, (CHUNK, WINDOW), 1) // SEG
    inside = (key_seg >= query_seg) & (key_seg <= query_seg + LEFT)
    line = jnp.dot(
        table_ref[layer_index] * LOG2_E, onehot, precision=lax.Precision.HIGHEST,
        preferred_element_type=f32,
    )
    for head in range(heads):
        spread = jnp.broadcast_to(line[head : head + 1, :], (CHUNK, LINE))
        rolled = pltpu.roll(spread, LINE - CHUNK + 1, 1, stride=1, stride_axis=0)
        tile_ref[head] = jnp.where(inside, rolled[:, :WINDOW], masked_score)


def attention_kernel(
    block, layer_index, q_start, row_start, step, starts, prior, q_ref, *refs,
):
    piece_refs = refs[:PIECES]
    tile_ref, wout_ref, *out_refs, mixed_ref = refs[PIECES:]
    heads = q_ref.shape[0]
    kv_width = q_ref.shape[2]
    group = heads * HEAD_DIM // kv_width
    count = mixed_ref.shape[0]
    rows = slice(q_start, q_start + count)

    pieces = [
        ref[start : start + CHUNK, :] for ref, start in zip(piece_refs, starts, strict=True)
    ]
    keys = jnp.concatenate([piece[:, :kv_width] for piece in pieces], axis=0)
    values = jnp.concatenate([piece[:, kv_width:] for piece in pieces], axis=0)
    values = jnp.concatenate([values, jnp.ones_like(values)], axis=1)
    key_index = lax.broadcasted_iota(jnp.int32, (1, WINDOW), 1)
    outside = (key_index < prior * CHUNK) & (lax.axis_index("sp") == 0)
    outside = jnp.where(outside, masked_score, 0.0)
    for first in range(0, heads, step):
        stacked = jnp.concatenate([q_ref[first + index, rows, :] for index in range(step)], axis=0)
        scores = lax.dot_general(
            stacked, keys, (((1,), (1,)), ((), ())), preferred_element_type=f32
        )
        expons = []
        for index in range(step):
            score = scores[index * count : (index + 1) * count, :]
            score = score + tile_ref[first + index, row_start : row_start + count, :]
            if prior:
                score = score + outside
            peak = jnp.max(score, axis=-1, keepdims=True)
            expons.append(jnp.exp2(score - peak).astype(bf16))
        summed = jnp.dot(
            jnp.concatenate(expons, axis=0), values, preferred_element_type=f32
        )
        ratio = summed[:, :kv_width] / summed[:, kv_width:]
        for index in range(step):
            at = (first + index) // group * HEAD_DIM
            into = (first + index) * HEAD_DIM
            part = ratio[index * count : (index + 1) * count, at : at + HEAD_DIM]
            mixed_ref[:, into : into + HEAD_DIM] = part.astype(bf16)

    out_projection(block, layer_index, mixed_ref, wout_ref, *out_refs)


def out_projection(block, layer_index, mixed_ref, wout_ref, keep_ref, send_ref=None):
    parity = lax.axis_index("tp") % 2
    mixed = mixed_ref[...]

    def project(place):
        cols = pl.ds(pl.multiple_of(place * block, LANES), block)
        value = jnp.dot(mixed, wout_ref[layer_index, :, cols], preferred_element_type=f32)
        return value.astype(bf16)

    if send_ref is None and keep_ref.shape[1] == block:
        chip = lax.axis_index("tp") // 2
        keep_ref[...] = project(2 * (1 - chip) + 1 - parity)
        return
    for index in range(keep_ref.shape[1] // block):
        into = slice(index * block, (index + 1) * block)
        if send_ref is None:
            keep_ref[:, into] = project(2 * index + 1 - parity)
        else:
            send_ref[:, into] = project(2 * index + 1 - parity)
            keep_ref[:, into] = project(2 * index + parity)


def keep_kernel(block, layer_index, mixed_ref, wout_ref, keep_ref):
    parity = lax.axis_index("tp") % 2
    mixed = mixed_ref[...]
    for index in range(keep_ref.shape[1] // block):
        cols = pl.ds(pl.multiple_of((2 * index + parity) * block, LANES), block)
        value = jnp.dot(mixed, wout_ref[layer_index, :, cols], preferred_element_type=f32)
        keep_ref[:, index * block : (index + 1) * block] = value.astype(bf16)


def project_kernel(block, layer_index, which, mixed_ref, wout_ref, *out_refs):
    parity = lax.axis_index("tp") % 2
    chip = lax.axis_index("tp") // 2
    mixed = mixed_ref[...]
    for (near_chip, near_core), target in zip(which, out_refs, strict=True):
        place = 2 * (chip if near_chip else 1 - chip) + (parity if near_core else 1 - parity)
        cols = pl.ds(pl.multiple_of(place * block, LANES), block)
        value = jnp.dot(mixed, wout_ref[layer_index, :, cols], preferred_element_type=f32)
        target[...] = value.astype(bf16)


def own_kernel(q_start, starts, q_ref, *refs):
    piece_refs = refs[: len(starts)]
    tile_ref, peak_ref, summed_ref = refs[len(starts) :]
    kv_width = q_ref.shape[2]
    rows = slice(q_start, q_start + CHUNK)
    pieces = [
        ref[start : start + CHUNK, :] for ref, start in zip(piece_refs, starts, strict=True)
    ]
    keys = jnp.concatenate([piece[:, :kv_width] for piece in pieces], axis=0)
    values = jnp.concatenate([piece[:, kv_width:] for piece in pieces], axis=0)
    values = jnp.concatenate([values, jnp.ones_like(values)], axis=1)
    lower = WINDOW - len(starts) * CHUNK
    heads = q_ref.shape[0]
    scores = lax.dot_general(
        q_ref[:, rows, :].reshape(heads * CHUNK, kv_width), keys, (((1,), (1,)), ((), ())),
        preferred_element_type=f32,
    ).reshape(heads, CHUNK, keys.shape[0])
    scores = scores + tile_ref[:, :, lower:]
    peaks = jnp.max(scores, axis=-1, keepdims=True)
    expons = jnp.exp2(scores - peaks).astype(bf16)
    peak_ref[...] = jnp.broadcast_to(peaks, peak_ref.shape)
    summed = jnp.dot(
        expons.reshape(heads * CHUNK, keys.shape[0]), values, preferred_element_type=f32
    )
    summed_ref[...] = summed.reshape(summed_ref.shape)


def joined_kernel(block, layer_index, q_start, starts, q_ref, *refs):
    piece_refs = refs[: len(starts)]
    tile_ref, peak_ref, summed_ref, wout_ref, *out_refs, mixed_ref = refs[len(starts) :]
    heads = q_ref.shape[0]
    kv_width = q_ref.shape[2]
    group = heads * HEAD_DIM // kv_width
    rows = slice(q_start, q_start + CHUNK)
    upper = len(starts) * CHUNK

    def put(head, summed):
        ratio = summed[:, :kv_width] / summed[:, kv_width:]
        at = head // group * HEAD_DIM
        into = head * HEAD_DIM
        mixed_ref[:, into : into + HEAD_DIM] = ratio[:, at : at + HEAD_DIM].astype(bf16)

    @pl.when(lax.axis_index("sp") == 0)
    def _():
        for head in range(heads):
            put(head, summed_ref[head])

    @pl.when(lax.axis_index("sp") > 0)
    def _():
        pieces = [
            ref[start : start + CHUNK, :] for ref, start in zip(piece_refs, starts, strict=True)
        ]
        keys = jnp.concatenate([piece[:, :kv_width] for piece in pieces], axis=0)
        values = jnp.concatenate([piece[:, kv_width:] for piece in pieces], axis=0)
        values = jnp.concatenate([values, jnp.ones_like(values)], axis=1)
        scores = lax.dot_general(
            q_ref[:, rows, :].reshape(heads * CHUNK, kv_width), keys, (((1,), (1,)), ((), ())),
            preferred_element_type=f32,
        ).reshape(heads, CHUNK, upper)
        scores = scores + tile_ref[:, :, :upper]
        before = peak_ref[...]
        peaks = jnp.max(scores, axis=-1, keepdims=True)
        peaks = jnp.maximum(before, jnp.broadcast_to(peaks, before.shape))
        spread = jnp.concatenate([peaks] * len(starts), axis=2)
        expons = jnp.exp2(scores - spread).astype(bf16)
        summed = jnp.dot(
            expons.reshape(heads * CHUNK, upper), values, preferred_element_type=f32
        ).reshape(summed_ref.shape)
        scale = jnp.exp2(before - peaks)
        for head in range(heads):
            wide = jnp.concatenate([scale[head]] * (summed.shape[2] // LANES), axis=1)
            put(head, summed_ref[head] * wide + summed[head])

    out_projection(block, layer_index, mixed_ref, wout_ref, *out_refs)


def add_kernel(a_ref, b_ref, out_ref):
    out_ref[...] = (a_ref[...].astype(f32) + b_ref[...].astype(f32)).astype(bf16)


def split_add_kernel(block, bit, a_ref, b_ref, keep_ref, send_ref):
    parity = (lax.axis_index("tp") >> bit) & 1
    for index in range(keep_ref.shape[1] // block):
        into = slice(index * block, (index + 1) * block)
        for target, side in ((send_ref, 1 - parity), (keep_ref, parity)):
            cols = pl.ds(pl.multiple_of((2 * index + side) * block, LANES), block)
            target[:, into] = (
                a_ref[:, cols].astype(f32) + b_ref[:, cols].astype(f32)
            ).astype(bf16)


def residual_kernel(block, start, x_ref, *refs):
    out_ref = refs[-1]
    parity = lax.axis_index("tp") % 2
    at = 0
    for a_ref, b_ref in zip(refs[:-1:2], refs[1:-1:2], strict=True):
        count = a_ref.shape[0]
        for index in range(out_ref.shape[1] // block):
            into = slice(index * block, (index + 1) * block)
            cols = pl.ds(pl.multiple_of((2 * index + parity) * block, LANES), block)
            added = a_ref[:, into].astype(f32) + b_ref[:, into].astype(f32)
            held = x_ref[start + at : start + at + count, cols].astype(f32)
            out_ref[at : at + count, into] = (held + added).astype(bf16)
        at += count


def result_kernel(block, places, *refs):
    out_hbm, held_ref, sems = refs[-3:]
    cols = pl.ds(pl.multiple_of((lax.axis_index("tp") // 2) * block, LANES), block)
    copies = []
    at = 0
    for index, (start, count, addends) in enumerate(places):
        added = sum(ref[...].astype(f32) for ref in refs[at + 1 : at + 1 + addends])
        held = refs[at][:, cols].astype(f32)
        held_ref[start : start + count, :] = (held + added).astype(bf16)
        span = pl.ds(start, count)
        copy = pltpu.make_async_copy(held_ref.at[span, :], out_hbm.at[span, :], sems.at[index])
        copy.start()
        copies.append(copy)
        at += 1 + addends
    for copy in copies:
        copy.wait()


def swapped(value, bit):
    size = lax.axis_size("tp")
    return lax.ppermute(value, "tp", [(d, d ^ (1 << bit)) for d in range(size)])


def passed_along(value, closed):
    size = lax.axis_size("sp")
    edges = [(d, (d + 1) % size) for d in range(size if closed else size - 1)]
    return lax.ppermute(value, "sp", edges)


def kept_in_hbm(*arrays):
    return [pltpu.with_memory_space_constraint(array, pltpu.HBM) for array in arrays]


def layers(stream, attn_gain, w_query, w_key, w_value, w_out, query_gain, key_gain, rel_bias):
    rows, width = stream.shape
    bits = lax.axis_size("tp").bit_length() - 1
    block = width // lax.axis_size("tp")
    half = width // 2
    query_width = w_query.shape[2]
    kv_width = w_key.shape[2]
    heads = query_width // HEAD_DIM
    parts = rows // CHUNK
    order = list(reversed(range(parts)))

    def queries(layer_index, normed, *ahead):
        count = normed.shape[0]
        return pl.pallas_call(
            functools.partial(query_kernel, layer_index),
            out_shape=out((heads, count, kv_width)),
            in_specs=[whole] * (3 + len(ahead)),
            out_specs=whole,
            compiler_params=params(),
            cost_estimate=cost(2e9, 2 * width * query_width),
            name="queries",
        )(normed, w_query, query_gain, *ahead)

    def attention_out(early, count):
        if early:
            return dict(
                out_shape=[out((count, early)), out((count, query_width))],
                out_specs=[whole, whole],
            )
        return dict(
            out_shape=[out((count, half))] * 2,
            out_specs=[whole, whole],
            scratch_shapes=[pltpu.VMEM((count, query_width), bf16)],
        )

    def attention(layer_index, part, inner, count, query, q_start, pieces, starts, early=0):
        return pl.pallas_call(
            functools.partial(
                attention_kernel, block, layer_index, q_start, inner,
                STEPS[count], starts, max(0, PIECES - 1 - part),
            ),
            **attention_out(early, count),
            in_specs=[whole] * (PIECES + 3),
            compiler_params=params(),
            cost_estimate=cost(
                2 * CHUNK * query_width * (width + 4 * WINDOW), 2 * width * query_width
            ),
            name="attention",
        )(query, *pieces, tiles[layer_index], w_out)

    def own_part(layer_index, part, query, q_start, pieces, starts):
        prior = max(0, PIECES - 1 - part)
        return pl.pallas_call(
            functools.partial(own_kernel, q_start, starts[prior:]),
            out_shape=[
                out((heads, CHUNK, LANES), f32), out((heads, CHUNK, 2 * kv_width), f32)
            ],
            in_specs=[whole] * (PIECES - prior + 2),
            out_specs=[whole, whole],
            compiler_params=params(),
            cost_estimate=cost(5e8, 1e6),
            name="own_part",
        )(query, *pieces[prior:], tiles[layer_index])

    def joined(layer_index, part, query, q_start, pieces, starts, own, early=0):
        prior = max(0, PIECES - 1 - part)
        return pl.pallas_call(
            functools.partial(joined_kernel, block, layer_index, q_start, starts[:prior]),
            **attention_out(early, CHUNK),
            in_specs=[whole] * (prior + 5),
            compiler_params=params(),
            cost_estimate=cost(1e9, 2 * width * query_width),
            name="joined",
        )(query, *pieces[:prior], tiles[layer_index], *own, w_out)

    def project(layer_index, mixed, which):
        return pl.pallas_call(
            functools.partial(project_kernel, block, layer_index, which),
            out_shape=[out((mixed.shape[0], block))] * len(which),
            in_specs=[whole, whole],
            out_specs=[whole] * len(which),
            compiler_params=params(),
            cost_estimate=cost(3e8, 1e6),
            name="project",
        )(mixed, w_out)

    def added(one, two):
        return pl.pallas_call(
            add_kernel,
            out_shape=out(one.shape),
            in_specs=[whole, whole],
            out_specs=whole,
            compiler_params=params(),
            name="add",
        )(one, two)

    last = parts - 1
    normed, kv, gains, weights, key_gains, table = pl.pallas_call(
        first_norm_kernel,
        out_shape=[
            out((CHUNK, width)), out((CHUNK, 2 * kv_width)),
            out(attn_gain.shape, f32), out((2, width, kv_width)),
            out(key_gain.shape, f32), out(rel_bias.shape, f32),
        ],
        in_specs=[in_hbm] * 6,
        out_specs=[whole] * 6,
        scratch_shapes=[
            pltpu.VMEM((CHUNK, width), bf16),
            pltpu.SemaphoreType.DMA((2,)),
            pltpu.SemaphoreType.DMA((6,)),
        ],
        compiler_params=params(),
        cost_estimate=cost(3e9, 4 * rows * width),
        name="norm_kv_first",
    )(*kept_in_hbm(stream, attn_gain, w_key, w_value, key_gain, rel_bias))
    found = pl.pallas_call(
        rest_norm_kernel,
        out_shape=[out((CHUNK, width))] * last + [out((CHUNK, 2 * kv_width))] * last,
        in_specs=[whole] * 4,
        out_specs=[whole] * (2 * last),
        compiler_params=params(),
        cost_estimate=cost(1e9, 4 * rows * width),
        name="norm_kv_rest",
    )(stream, gains, weights, key_gains)
    normeds_first = [*found[:last], normed]
    kvs_first = [*found[last:], kv]
    first_priors = {}
    for part in order[: PIECES - 1]:
        first_priors[part - parts] = passed_along(kvs_first[part], True)
    tiles = []
    for layer_index in range(LAYERS):
        tiles.append(
            pl.pallas_call(
                functools.partial(bias_kernel, layer_index),
                out_shape=out((heads, CHUNK, WINDOW), f32),
                in_specs=[whole] * (2 - layer_index),
                out_specs=whole,
                compiler_params=params(),
                cost_estimate=cost(2e9, 1e6),
                name="bias_tiles",
            )(table, *[w_query] * (1 - layer_index))
        )

    mine, other, kvs, normeds = {}, {}, {}, {}
    for part in order:
        query = queries(0, normeds_first[part], *[w_out] * (part == last))
        pieces, starts = [], [0] * PIECES
        for index in range(PIECES):
            behind = part - (PIECES - 1) + index
            pieces.append(first_priors[behind] if behind < 0 else kvs_first[behind])
        sums = []
        for inner, count in split_rows(False):
            if part < PIECES - 1:
                own = own_part(0, part, query, 0, pieces, starts)
                send, mixed = joined(
                    0, part, query, 0, pieces, starts, own, half
                )
                keep = pl.pallas_call(
                    functools.partial(keep_kernel, block, 0),
                    out_shape=out((CHUNK, half)),
                    in_specs=[whole, whole],
                    out_specs=whole,
                    compiler_params=params(),
                    cost_estimate=cost(3e8, 1e6),
                    name="keep",
                )(mixed, w_out)
            else:
                keep, send = attention(
                    0, part, inner, count, query, inner, pieces, starts
                )
            received = swapped(send, 0)
            for bit in range(1, bits):
                summed = added(keep, received)
                keep, received = summed, swapped(summed, bit)
            sums += [keep, received]
        mine[part] = pl.pallas_call(
            functools.partial(residual_kernel, block, part * CHUNK),
            out_shape=out((CHUNK, half)),
            in_specs=[whole] * (1 + len(sums)),
            out_specs=whole,
            compiler_params=params(),
            name="residual",
        )(stream, *sums)
        other[part] = swapped(mine[part], 0)

    priors = {}
    for part in order:
        normeds[part], kvs[part] = pl.pallas_call(
            functools.partial(next_norm_kernel, 1, block),
            out_shape=[out((CHUNK, width)), out((CHUNK, 2 * kv_width))],
            in_specs=[whole] * 6,
            out_specs=[whole, whole],
            compiler_params=params(),
            cost_estimate=cost(4 * CHUNK * width * kv_width, 4 * CHUNK * width),
            name="norm_kv_next",
        )(mine[part], other[part], attn_gain, w_key, w_value, key_gain)
        if part >= parts - (PIECES - 1):
            priors[part - parts] = passed_along(kvs[part], True)

    places, outs = [], []
    for part in order:
        query = queries(1, normeds[part])
        pieces = []
        for index in range(PIECES):
            behind = part - (PIECES - 1) + index
            pieces.append(priors[behind] if behind < 0 else kvs[behind])
        early = block if bits == 2 and part == 0 else 0
        if part == 0:
            own = own_part(1, part, query, 0, pieces, [0] * PIECES)
            keep, send = joined(1, part, query, 0, pieces, [0] * PIECES, own, early)
        else:
            keep, send = attention(
                1, part, 0, CHUNK, query, 0, pieces, [0] * PIECES, early
            )
        if early:
            first, mixed = keep, send
            received = swapped(first, 0)
            send = project(1, mixed, ((False, True),))[0]
            summed = added(send, received)
            received = swapped(summed, 1)
            keep, other = project(1, mixed, ((True, True), (True, False)))
            aside = swapped(other, 0)
            addends = [keep, aside, received]
        else:
            received = swapped(send, 0)
            for bit in range(1, bits):
                left = keep.shape[1] // 2
                keep, send = pl.pallas_call(
                    functools.partial(split_add_kernel, block, bit),
                    out_shape=[out((CHUNK, left))] * 2,
                    in_specs=[whole, whole],
                    out_specs=[whole, whole],
                    compiler_params=params(),
                    name="split_add",
                )(keep, received)
                received = swapped(send, bit)
            addends = [keep, received]
        places.append((part * CHUNK, CHUNK, len(addends)))
        outs += [mine[part], *addends]

    return pl.pallas_call(
        functools.partial(result_kernel, block, places),
        out_shape=out((rows, block)),
        in_specs=[whole] * len(outs),
        out_specs=in_hbm,
        scratch_shapes=[pltpu.VMEM((rows, block), bf16), pltpu.SemaphoreType.DMA((len(places),))],
        compiler_params=params(),
        name="result",
    )(*outs)


def split_rows(fine):
    return [(at, SEG) for at in range(0, CHUNK, SEG)] if fine else [(0, CHUNK)]


STEPS = {CHUNK: 1, SEG: 2}


def solution(mesh):
    return jax.shard_map(
        layers,
        mesh=mesh,
        in_specs=(
            P("sp", None),
            P(),
            P(None, None, "tp"),
            P(None, None, "tp"),
            P(None, None, "tp"),
            P(None, "tp", None),
            P(),
            P(),
            P(None, "tp", None),
        ),
        out_specs=P("sp", "tp"),
        check_vma=False,
    )
```

```python
import functools

import jax
import jax.numpy as jnp
from jax import lax
from jax.experimental import pallas as pl
from jax.experimental.pallas import tpu as pltpu
from jax.sharding import PartitionSpec as P


HEAD_DIM = 64
SEG = 64
LEFT = 4
CLIP = 128
LAYERS = 2

REACH = LEFT * SEG
CHUNK = 2 * SEG
PIECES = REACH // CHUNK + 1
WINDOW = REACH + CHUNK
LINE = WINDOW + CHUNK
LANES = 128

norm_eps = 1e-06
masked_score = -1e30

LOG2_E = 1.4426950408889634

bf16 = jnp.bfloat16
f32 = jnp.float32

whole = pl.BlockSpec(memory_space=pltpu.VMEM)
in_hbm = pl.BlockSpec(memory_space=pltpu.HBM)


def params():
    return pltpu.CompilerParams(vmem_limit_bytes=12 * 1024 * 1024)


def cost(flops, moved):
    return pl.CostEstimate(flops=int(flops), bytes_accessed=int(moved), transcendentals=0)


def out(shape, dtype=bf16):
    return jax.ShapeDtypeStruct(shape, dtype)


def head_norm(flat, gain_row):
    width = flat.shape[1]
    step = min(width, LANES)
    row = lax.broadcasted_iota(jnp.int32, (step, step), 0) // HEAD_DIM
    col = lax.broadcasted_iota(jnp.int32, (step, step), 1) // HEAD_DIM
    mean_of = jnp.where(row == col, 1.0 / HEAD_DIM, 0.0).astype(bf16)
    gain = jnp.concatenate([gain_row] * (step // HEAD_DIM), axis=1)
    pieces = []
    for lower in range(0, width, step):
        part = flat[:, lower : lower + step]
        squared = part * part
        high = squared.astype(bf16)
        low = (squared - high.astype(f32)).astype(bf16)
        mean = jnp.dot(high, mean_of, preferred_element_type=f32) + jnp.dot(
            low, mean_of, preferred_element_type=f32
        )
        pieces.append(part * lax.rsqrt(mean + norm_eps) * gain)
    return pieces


def key_value_body(normed, weights, key_gain_row, kv_refs):
    flat = jnp.dot(normed, weights, preferred_element_type=f32)
    kv_width = flat.shape[1] // 2
    keys = head_norm(flat[:, :kv_width], key_gain_row)[0]
    values = flat[:, kv_width:]
    both = jnp.concatenate([keys, values], axis=1).astype(bf16)
    for index, kv_ref in enumerate(kv_refs):
        kv_ref[...] = both[index * CHUNK : (index + 1) * CHUNK, :]


def first_norm_kernel(
    x_hbm, gain_hbm, wk_hbm, wv_hbm, kg_hbm, table_hbm,
    normed_ref, kv_ref, gain_ref, weight_ref, kg_ref, table_ref,
    x_ref, row_sems, sems,
):
    steps = row_sems.shape[0]
    rest = x_hbm.shape[0] - x_ref.shape[0]
    share = x_ref.shape[0] // steps
    row_copies = []
    for index in range(steps):
        at = pl.ds(index * share, share)
        source = x_hbm.at[pl.ds(rest + index * share, share), :]
        row_copies.append(
            pltpu.make_async_copy(source, x_ref.at[at, :], row_sems.at[index])
        )
    gain_copy = pltpu.make_async_copy(gain_hbm, gain_ref, sems.at[0])
    weight_copies = [
        pltpu.make_async_copy(wk_hbm.at[0], weight_ref.at[0], sems.at[1]),
        pltpu.make_async_copy(wv_hbm.at[0], weight_ref.at[1], sems.at[2]),
        pltpu.make_async_copy(kg_hbm, kg_ref, sems.at[3]),
    ]
    late = [
        pltpu.make_async_copy(table_hbm, table_ref, sems.at[4]),
    ]
    for copy in [gain_copy] + row_copies + weight_copies + late:
        copy.start()
    gain_copy.wait()
    gain = gain_ref[0:1, :]
    for index, copy in enumerate(row_copies):
        copy.wait()
        at = slice(index * share, (index + 1) * share)
        normed_ref[at, :] = normalized(x_ref[at, :], gain)
    for copy in weight_copies:
        copy.wait()
    weights = jnp.concatenate([weight_ref[0], weight_ref[1]], axis=1)
    key_value_body(normed_ref[...], weights, kg_ref[0:1, :], [kv_ref])
    for copy in late:
        copy.wait()


def normalized(rows, gain):
    current = rows.astype(f32)
    mean = jnp.mean(current * current, axis=-1, keepdims=True)
    return (current * lax.rsqrt(mean + norm_eps) * gain).astype(bf16)


def rest_norm_kernel(x_ref, gain_ref, weight_ref, kg_ref, *refs):
    parts = len(refs) // 2
    weights = jnp.concatenate([weight_ref[0], weight_ref[1]], axis=1)
    for index in range(parts):
        at = slice(index * CHUNK, (index + 1) * CHUNK)
        refs[index][...] = normalized(x_ref[at, :], gain_ref[0:1, :])
        key_value_body(refs[index][...], weights, kg_ref[0:1, :], [refs[parts + index]])


def next_norm_kernel(
    layer_index, block, mine_ref, other_ref, gain_ref, wk_ref, wv_ref, kg_ref,
    normed_ref, kv_ref,
):
    parity = lax.axis_index("tp") % 2
    mine = mine_ref[...].astype(f32)
    other = other_ref[...].astype(f32)
    total = jnp.sum(mine * mine, axis=-1, keepdims=True)
    total = total + jnp.sum(other * other, axis=-1, keepdims=True)
    scale = lax.rsqrt(total / (2 * mine.shape[1]) + norm_eps)
    for index in range(mine.shape[1] // block):
        for held, side in ((mine, parity), (other, 1 - parity)):
            cols = pl.ds(pl.multiple_of((2 * index + side) * block, LANES), block)
            piece = held[:, index * block : (index + 1) * block]
            gain = gain_ref[layer_index : layer_index + 1, cols]
            normed_ref[:, cols] = (piece * scale * gain).astype(bf16)
    key_value_body(
        normed_ref[...],
        jnp.concatenate([wk_ref[layer_index], wv_ref[layer_index]], axis=1),
        kg_ref[layer_index : layer_index + 1, :], [kv_ref],
    )


def query_kernel(layer_index, normed_ref, wq_ref, qg_ref, *refs):
    q_ref = refs[-1]
    flat = jnp.dot(normed_ref[...], wq_ref[layer_index], preferred_element_type=f32)
    query_body(flat, qg_ref[layer_index : layer_index + 1, :], q_ref)


def query_body(flat, gain_row, q_ref):
    pieces = head_norm(flat, gain_row * (HEAD_DIM**-0.5 * LOG2_E))
    kv_width = q_ref.shape[2]
    group = q_ref.shape[0] * HEAD_DIM // kv_width
    lanes = pieces[0].shape[1]
    for head in range(q_ref.shape[0]):
        at = head * HEAD_DIM
        piece = pieces[at // lanes][:, at % lanes : at % lanes + HEAD_DIM]
        before = head // group * HEAD_DIM
        after = kv_width - HEAD_DIM - before
        rows = piece.shape[0]
        spread = [jnp.zeros((rows, before), f32)] if before else []
        spread += [piece] + ([jnp.zeros((rows, after), f32)] if after else [])
        q_ref[head] = jnp.concatenate(spread, axis=1).astype(bf16)


def bias_kernel(layer_index, table_ref, *refs):
    tile_ref = refs[-1]
    heads, entries = table_ref.shape[1:]
    source = lax.broadcasted_iota(jnp.int32, (entries, LINE), 0)
    offset = lax.broadcasted_iota(jnp.int32, (entries, LINE), 1)
    distance = jnp.clip(WINDOW - 1 - offset, -CLIP, CLIP) + CLIP
    onehot = (source == distance).astype(f32)
    query_seg = lax.broadcasted_iota(jnp.int32, (CHUNK, WINDOW), 0) // SEG
    key_seg = lax.broadcasted_iota(jnp.int32, (CHUNK, WINDOW), 1) // SEG
    inside = (key_seg >= query_seg) & (key_seg <= query_seg + LEFT)
    line = jnp.dot(
        table_ref[layer_index] * LOG2_E, onehot, precision=lax.Precision.HIGHEST,
        preferred_element_type=f32,
    )
    for head in range(heads):
        spread = jnp.broadcast_to(line[head : head + 1, :], (CHUNK, LINE))
        rolled = pltpu.roll(spread, LINE - CHUNK + 1, 1, stride=1, stride_axis=0)
        tile_ref[head] = jnp.where(inside, rolled[:, :WINDOW], masked_score)


def attention_kernel(
    block, layer_index, q_start, row_start, step, starts, prior, q_ref, *refs,
):
    piece_refs = refs[:PIECES]
    tile_ref, wout_ref, *out_refs, mixed_ref = refs[PIECES:]
    heads = q_ref.shape[0]
    kv_width = q_ref.shape[2]
    group = heads * HEAD_DIM // kv_width
    count = mixed_ref.shape[0]
    rows = slice(q_start, q_start + count)

    pieces = [
        ref[start : start + CHUNK, :] for ref, start in zip(piece_refs, starts, strict=True)
    ]
    keys = jnp.concatenate([piece[:, :kv_width] for piece in pieces], axis=0)
    values = jnp.concatenate([piece[:, kv_width:] for piece in pieces], axis=0)
    values = jnp.concatenate([values, jnp.ones_like(values)], axis=1)
    key_index = lax.broadcasted_iota(jnp.int32, (1, WINDOW), 1)
    outside = (key_index < prior * CHUNK) & (lax.axis_index("sp") == 0)
    outside = jnp.where(outside, masked_score, 0.0)
    for first in range(0, heads, step):
        stacked = jnp.concatenate([q_ref[first + index, rows, :] for index in range(step)], axis=0)
        scores = lax.dot_general(
            stacked, keys, (((1,), (1,)), ((), ())), preferred_element_type=f32
        )
        expons = []
        for index in range(step):
            score = scores[index * count : (index + 1) * count, :]
            score = score + tile_ref[first + index, row_start : row_start + count, :]
            if prior:
                score = score + outside
            peak = jnp.max(score, axis=-1, keepdims=True)
            expons.append(jnp.exp2(score - peak).astype(bf16))
        summed = jnp.dot(
            jnp.concatenate(expons, axis=0), values, preferred_element_type=f32
        )
        ratio = summed[:, :kv_width] / summed[:, kv_width:]
        for index in range(step):
            at = (first + index) // group * HEAD_DIM
            into = (first + index) * HEAD_DIM
            part = ratio[index * count : (index + 1) * count, at : at + HEAD_DIM]
            mixed_ref[:, into : into + HEAD_DIM] = part.astype(bf16)

    out_projection(block, layer_index, mixed_ref, wout_ref, *out_refs)


def out_projection(block, layer_index, mixed_ref, wout_ref, keep_ref, send_ref=None):
    parity = lax.axis_index("tp") % 2
    mixed = mixed_ref[...]

    def project(place):
        cols = pl.ds(pl.multiple_of(place * block, LANES), block)
        value = jnp.dot(mixed, wout_ref[layer_index, :, cols], preferred_element_type=f32)
        return value.astype(bf16)

    if send_ref is None and keep_ref.shape[1] == block:
        chip = lax.axis_index("tp") // 2
        keep_ref[...] = project(2 * (1 - chip) + 1 - parity)
        return
    for index in range(keep_ref.shape[1] // block):
        into = slice(index * block, (index + 1) * block)
        if send_ref is None:
            keep_ref[:, into] = project(2 * index + 1 - parity)
        else:
            send_ref[:, into] = project(2 * index + 1 - parity)
            keep_ref[:, into] = project(2 * index + parity)


def keep_kernel(block, layer_index, mixed_ref, wout_ref, keep_ref):
    parity = lax.axis_index("tp") % 2
    mixed = mixed_ref[...]
    for index in range(keep_ref.shape[1] // block):
        cols = pl.ds(pl.multiple_of((2 * index + parity) * block, LANES), block)
        value = jnp.dot(mixed, wout_ref[layer_index, :, cols], preferred_element_type=f32)
        keep_ref[:, index * block : (index + 1) * block] = value.astype(bf16)


def project_kernel(block, layer_index, which, mixed_ref, wout_ref, *out_refs):
    parity = lax.axis_index("tp") % 2
    chip = lax.axis_index("tp") // 2
    mixed = mixed_ref[...]
    for (near_chip, near_core), target in zip(which, out_refs, strict=True):
        place = 2 * (chip if near_chip else 1 - chip) + (parity if near_core else 1 - parity)
        cols = pl.ds(pl.multiple_of(place * block, LANES), block)
        value = jnp.dot(mixed, wout_ref[layer_index, :, cols], preferred_element_type=f32)
        target[...] = value.astype(bf16)


def own_kernel(q_start, starts, q_ref, *refs):
    piece_refs = refs[: len(starts)]
    tile_ref, peak_ref, summed_ref = refs[len(starts) :]
    kv_width = q_ref.shape[2]
    rows = slice(q_start, q_start + CHUNK)
    pieces = [
        ref[start : start + CHUNK, :] for ref, start in zip(piece_refs, starts, strict=True)
    ]
    keys = jnp.concatenate([piece[:, :kv_width] for piece in pieces], axis=0)
    values = jnp.concatenate([piece[:, kv_width:] for piece in pieces], axis=0)
    values = jnp.concatenate([values, jnp.ones_like(values)], axis=1)
    lower = WINDOW - len(starts) * CHUNK
    heads = q_ref.shape[0]
    scores = lax.dot_general(
        q_ref[:, rows, :].reshape(heads * CHUNK, kv_width), keys, (((1,), (1,)), ((), ())),
        preferred_element_type=f32,
    ).reshape(heads, CHUNK, keys.shape[0])
    scores = scores + tile_ref[:, :, lower:]
    peaks = jnp.max(scores, axis=-1, keepdims=True)
    expons = jnp.exp2(scores - peaks).astype(bf16)
    peak_ref[...] = jnp.broadcast_to(peaks, peak_ref.shape)
    summed = jnp.dot(
        expons.reshape(heads * CHUNK, keys.shape[0]), values, preferred_element_type=f32
    )
    summed_ref[...] = summed.reshape(summed_ref.shape)


def joined_kernel(block, layer_index, q_start, starts, prior, q_ref, *refs):
    piece_refs = refs[: len(starts)]
    tile_ref, peak_ref, summed_ref, wout_ref, *out_refs, mixed_ref = refs[len(starts) :]
    heads = q_ref.shape[0]
    kv_width = q_ref.shape[2]
    group = heads * HEAD_DIM // kv_width
    rows = slice(q_start, q_start + CHUNK)
    upper = len(starts) * CHUNK

    def put(head, summed):
        ratio = summed[:, :kv_width] / summed[:, kv_width:]
        at = head // group * HEAD_DIM
        into = head * HEAD_DIM
        mixed_ref[:, into : into + HEAD_DIM] = ratio[:, at : at + HEAD_DIM].astype(bf16)

    def join():
        pieces = [
            ref[start : start + CHUNK, :] for ref, start in zip(piece_refs, starts, strict=True)
        ]
        keys = jnp.concatenate([piece[:, :kv_width] for piece in pieces], axis=0)
        values = jnp.concatenate([piece[:, kv_width:] for piece in pieces], axis=0)
        values = jnp.concatenate([values, jnp.ones_like(values)], axis=1)
        scores = lax.dot_general(
            q_ref[:, rows, :].reshape(heads * CHUNK, kv_width), keys, (((1,), (1,)), ((), ())),
            preferred_element_type=f32,
        ).reshape(heads, CHUNK, upper)
        scores = scores + tile_ref[:, :, :upper]
        if prior < len(starts):
            lane = lax.broadcasted_iota(jnp.int32, (1, 1, upper), 2)
            outside = (lane < prior * CHUNK) & (lax.axis_index("sp") == 0)
            scores = scores + jnp.where(outside, masked_score, 0.0)
        before = peak_ref[...]
        peaks = jnp.max(scores, axis=-1, keepdims=True)
        peaks = jnp.maximum(before, jnp.broadcast_to(peaks, before.shape))
        spread = jnp.concatenate([peaks] * len(starts), axis=2)
        expons = jnp.exp2(scores - spread).astype(bf16)
        summed = jnp.dot(
            expons.reshape(heads * CHUNK, upper), values, preferred_element_type=f32
        ).reshape(summed_ref.shape)
        scale = jnp.exp2(before - peaks)
        for head in range(heads):
            wide = jnp.concatenate([scale[head]] * (summed.shape[2] // LANES), axis=1)
            put(head, summed_ref[head] * wide + summed[head])

    if prior < len(starts):
        join()
    else:
        pl.when(lax.axis_index("sp") > 0)(join)

        @pl.when(lax.axis_index("sp") == 0)
        def _():
            for head in range(heads):
                put(head, summed_ref[head])

    out_projection(block, layer_index, mixed_ref, wout_ref, *out_refs)


def add_kernel(a_ref, b_ref, out_ref):
    out_ref[...] = (a_ref[...].astype(f32) + b_ref[...].astype(f32)).astype(bf16)


def split_add_kernel(block, bit, a_ref, b_ref, keep_ref, send_ref):
    parity = (lax.axis_index("tp") >> bit) & 1
    for index in range(keep_ref.shape[1] // block):
        into = slice(index * block, (index + 1) * block)
        for target, side in ((send_ref, 1 - parity), (keep_ref, parity)):
            cols = pl.ds(pl.multiple_of((2 * index + side) * block, LANES), block)
            target[:, into] = (
                a_ref[:, cols].astype(f32) + b_ref[:, cols].astype(f32)
            ).astype(bf16)


def residual_kernel(block, start, x_ref, *refs):
    out_ref = refs[-1]
    parity = lax.axis_index("tp") % 2
    at = 0
    for a_ref, b_ref in zip(refs[:-1:2], refs[1:-1:2], strict=True):
        count = a_ref.shape[0]
        for index in range(out_ref.shape[1] // block):
            into = slice(index * block, (index + 1) * block)
            cols = pl.ds(pl.multiple_of((2 * index + parity) * block, LANES), block)
            added = a_ref[:, into].astype(f32) + b_ref[:, into].astype(f32)
            held = x_ref[start + at : start + at + count, cols].astype(f32)
            out_ref[at : at + count, into] = (held + added).astype(bf16)
        at += count


def result_kernel(block, places, *refs):
    out_hbm, held_ref, sems = refs[-3:]
    cols = pl.ds(pl.multiple_of((lax.axis_index("tp") // 2) * block, LANES), block)
    copies = []
    at = 0
    for index, (start, count, addends) in enumerate(places):
        added = sum(ref[...].astype(f32) for ref in refs[at + 1 : at + 1 + addends])
        held = refs[at][:, cols].astype(f32)
        held_ref[start : start + count, :] = (held + added).astype(bf16)
        span = pl.ds(start, count)
        copy = pltpu.make_async_copy(held_ref.at[span, :], out_hbm.at[span, :], sems.at[index])
        copy.start()
        copies.append(copy)
        at += 1 + addends
    for copy in copies:
        copy.wait()


def swapped(value, bit):
    size = lax.axis_size("tp")
    return lax.ppermute(value, "tp", [(d, d ^ (1 << bit)) for d in range(size)])


def passed_along(value, closed):
    size = lax.axis_size("sp")
    edges = [(d, (d + 1) % size) for d in range(size if closed else size - 1)]
    return lax.ppermute(value, "sp", edges)


def kept_in_hbm(*arrays):
    return [pltpu.with_memory_space_constraint(array, pltpu.HBM) for array in arrays]


def layers(stream, attn_gain, w_query, w_key, w_value, w_out, query_gain, key_gain, rel_bias):
    rows, width = stream.shape
    bits = lax.axis_size("tp").bit_length() - 1
    block = width // lax.axis_size("tp")
    half = width // 2
    query_width = w_query.shape[2]
    kv_width = w_key.shape[2]
    heads = query_width // HEAD_DIM
    parts = rows // CHUNK
    order = list(reversed(range(parts)))

    def queries(layer_index, normed, *ahead):
        count = normed.shape[0]
        return pl.pallas_call(
            functools.partial(query_kernel, layer_index),
            out_shape=out((heads, count, kv_width)),
            in_specs=[whole] * (3 + len(ahead)),
            out_specs=whole,
            compiler_params=params(),
            cost_estimate=cost(2e9, 2 * width * query_width),
            name="queries",
        )(normed, w_query, query_gain, *ahead)

    def attention_out(early, count):
        if early:
            return dict(
                out_shape=[out((count, early)), out((count, query_width))],
                out_specs=[whole, whole],
            )
        return dict(
            out_shape=[out((count, half))] * 2,
            out_specs=[whole, whole],
            scratch_shapes=[pltpu.VMEM((count, query_width), bf16)],
        )

    def attention(layer_index, part, inner, count, query, q_start, pieces, starts, early=0):
        return pl.pallas_call(
            functools.partial(
                attention_kernel, block, layer_index, q_start, inner,
                STEPS[count], starts, max(0, PIECES - 1 - part),
            ),
            **attention_out(early, count),
            in_specs=[whole] * (PIECES + 3),
            compiler_params=params(),
            cost_estimate=cost(
                2 * CHUNK * query_width * (width + 4 * WINDOW), 2 * width * query_width
            ),
            name="attention",
        )(query, *pieces, tiles[layer_index], w_out)

    def own_part(layer_index, part, query, q_start, pieces, starts, late=None):
        prior = max(0, PIECES - 1 - part) if late is None else late
        return pl.pallas_call(
            functools.partial(own_kernel, q_start, starts[prior:]),
            out_shape=[
                out((heads, CHUNK, LANES), f32), out((heads, CHUNK, 2 * kv_width), f32)
            ],
            in_specs=[whole] * (PIECES - prior + 2),
            out_specs=[whole, whole],
            compiler_params=params(),
            cost_estimate=cost(5e8, 1e6),
            name="own_part",
        )(query, *pieces[prior:], tiles[layer_index])

    def joined(layer_index, part, query, q_start, pieces, starts, own, early=0, late=None):
        prior = max(0, PIECES - 1 - part)
        late = prior if late is None else late
        return pl.pallas_call(
            functools.partial(
                joined_kernel, block, layer_index, q_start, starts[:late], prior
            ),
            **attention_out(early, CHUNK),
            in_specs=[whole] * (late + 5),
            compiler_params=params(),
            cost_estimate=cost(1e9, 2 * width * query_width),
            name="joined",
        )(query, *pieces[:late], tiles[layer_index], *own, w_out)

    def project(layer_index, mixed, which):
        return pl.pallas_call(
            functools.partial(project_kernel, block, layer_index, which),
            out_shape=[out((mixed.shape[0], block))] * len(which),
            in_specs=[whole, whole],
            out_specs=[whole] * len(which),
            compiler_params=params(),
            cost_estimate=cost(3e8, 1e6),
            name="project",
        )(mixed, w_out)

    def added(one, two):
        return pl.pallas_call(
            add_kernel,
            out_shape=out(one.shape),
            in_specs=[whole, whole],
            out_specs=whole,
            compiler_params=params(),
            name="add",
        )(one, two)

    last = parts - 1
    normed, kv, gains, weights, key_gains, table = pl.pallas_call(
        first_norm_kernel,
        out_shape=[
            out((CHUNK, width)), out((CHUNK, 2 * kv_width)),
            out(attn_gain.shape, f32), out((2, width, kv_width)),
            out(key_gain.shape, f32), out(rel_bias.shape, f32),
        ],
        in_specs=[in_hbm] * 6,
        out_specs=[whole] * 6,
        scratch_shapes=[
            pltpu.VMEM((CHUNK, width), bf16),
            pltpu.SemaphoreType.DMA((2,)),
            pltpu.SemaphoreType.DMA((6,)),
        ],
        compiler_params=params(),
        cost_estimate=cost(3e9, 4 * rows * width),
        name="norm_kv_first",
    )(*kept_in_hbm(stream, attn_gain, w_key, w_value, key_gain, rel_bias))
    found = pl.pallas_call(
        rest_norm_kernel,
        out_shape=[out((CHUNK, width))] * last + [out((CHUNK, 2 * kv_width))] * last,
        in_specs=[whole] * 4,
        out_specs=[whole] * (2 * last),
        compiler_params=params(),
        cost_estimate=cost(1e9, 4 * rows * width),
        name="norm_kv_rest",
    )(stream, gains, weights, key_gains)
    normeds_first = [*found[:last], normed]
    kvs_first = [*found[last:], kv]
    first_priors = {}
    for part in order[: PIECES - 1]:
        first_priors[part - parts] = passed_along(kvs_first[part], True)
    tiles = []
    for layer_index in range(LAYERS):
        tiles.append(
            pl.pallas_call(
                functools.partial(bias_kernel, layer_index),
                out_shape=out((heads, CHUNK, WINDOW), f32),
                in_specs=[whole],
                out_specs=whole,
                compiler_params=params(),
                cost_estimate=cost(2e9, 1e6),
                name="bias_tiles",
            )(table)
        )

    mine, other, kvs, normeds = {}, {}, {}, {}
    for part in order:
        query = queries(0, normeds_first[part], *[w_out] * (part == last))
        pieces, starts = [], [0] * PIECES
        for index in range(PIECES):
            behind = part - (PIECES - 1) + index
            pieces.append(first_priors[behind] if behind < 0 else kvs_first[behind])
        sums = []
        for inner, count in split_rows(False):
            if part < PIECES - 1:
                own = own_part(0, part, query, 0, pieces, starts)
                send, mixed = joined(
                    0, part, query, 0, pieces, starts, own, half
                )
                keep = pl.pallas_call(
                    functools.partial(keep_kernel, block, 0),
                    out_shape=out((CHUNK, half)),
                    in_specs=[whole, whole],
                    out_specs=whole,
                    compiler_params=params(),
                    cost_estimate=cost(3e8, 1e6),
                    name="keep",
                )(mixed, w_out)
            else:
                keep, send = attention(
                    0, part, inner, count, query, inner, pieces, starts
                )
            received = swapped(send, 0)
            for bit in range(1, bits):
                summed = added(keep, received)
                keep, received = summed, swapped(summed, bit)
            sums += [keep, received]
        mine[part] = pl.pallas_call(
            functools.partial(residual_kernel, block, part * CHUNK),
            out_shape=out((CHUNK, half)),
            in_specs=[whole] * (1 + len(sums)),
            out_specs=whole,
            compiler_params=params(),
            name="residual",
        )(stream, *sums)
        other[part] = swapped(mine[part], 0)

    priors = {}
    for part in order:
        normeds[part], kvs[part] = pl.pallas_call(
            functools.partial(next_norm_kernel, 1, block),
            out_shape=[out((CHUNK, width)), out((CHUNK, 2 * kv_width))],
            in_specs=[whole] * 6,
            out_specs=[whole, whole],
            compiler_params=params(),
            cost_estimate=cost(4 * CHUNK * width * kv_width, 4 * CHUNK * width),
            name="norm_kv_next",
        )(mine[part], other[part], attn_gain, w_key, w_value, key_gain)
        if part >= parts - (PIECES - 1):
            priors[part - parts] = passed_along(kvs[part], True)

    places, outs = [], []
    for part in order:
        query = queries(1, normeds[part])
        pieces = []
        for index in range(PIECES):
            behind = part - (PIECES - 1) + index
            pieces.append(priors[behind] if behind < 0 else kvs[behind])
        early = block if bits == 2 and part == 0 else 0
        if part == 0:
            own = own_part(1, part, query, 0, pieces, [0] * PIECES)
            keep, send = joined(1, part, query, 0, pieces, [0] * PIECES, own, early)
        elif part == order[0]:
            late = PIECES - 1
            own = own_part(1, part, query, 0, pieces, [0] * PIECES, late)
            keep, send = joined(
                1, part, query, 0, pieces, [0] * PIECES, own, early, late
            )
        else:
            keep, send = attention(
                1, part, 0, CHUNK, query, 0, pieces, [0] * PIECES, early
            )
        if early:
            first, mixed = keep, send
            received = swapped(first, 0)
            send = project(1, mixed, ((False, True),))[0]
            summed = added(send, received)
            received = swapped(summed, 1)
            keep, other = project(1, mixed, ((True, True), (True, False)))
            aside = swapped(other, 0)
            addends = [keep, aside, received]
        else:
            received = swapped(send, 0)
            for bit in range(1, bits):
                left = keep.shape[1] // 2
                keep, send = pl.pallas_call(
                    functools.partial(split_add_kernel, block, bit),
                    out_shape=[out((CHUNK, left))] * 2,
                    in_specs=[whole, whole],
                    out_specs=[whole, whole],
                    compiler_params=params(),
                    name="split_add",
                )(keep, received)
                received = swapped(send, bit)
            addends = [keep, received]
        places.append((part * CHUNK, CHUNK, len(addends)))
        outs += [mine[part], *addends]

    return pl.pallas_call(
        functools.partial(result_kernel, block, places),
        out_shape=out((rows, block)),
        in_specs=[whole] * len(outs),
        out_specs=in_hbm,
        scratch_shapes=[pltpu.VMEM((rows, block), bf16), pltpu.SemaphoreType.DMA((len(places),))],
        compiler_params=params(),
        name="result",
    )(*outs)


def split_rows(fine):
    return [(at, SEG) for at in range(0, CHUNK, SEG)] if fine else [(0, CHUNK)]


STEPS = {CHUNK: 1, SEG: 2}


def solution(mesh):
    return jax.shard_map(
        layers,
        mesh=mesh,
        in_specs=(
            P("sp", None),
            P(),
            P(None, None, "tp"),
            P(None, None, "tp"),
            P(None, None, "tp"),
            P(None, "tp", None),
            P(),
            P(),
            P(None, "tp", None),
        ),
        out_specs=P("sp", "tp"),
        check_vma=False,
    )
```
